512 devices in a mesh: fs: 64 (over z, y), tp: 8 (over x, core).
Axes of the slice: x: 4, y: 4, z: 16, core: 2. Of those that a mesh axis runs over, the one named last changes fastest.
Arguments:
- block_input: bfloat16 [65536, 2048], P('fs'), may hold values from -6 to 6
- value_cotangent: bfloat16 [65536, 1024], P('fs', 'tp'), may hold values from -6 to 6
- mixed_output: bfloat16 [65536, 1024], P('fs', 'tp'), may hold values from -6 to 6
- output_cotangent: bfloat16 [65536, 2048], P('fs'), may hold values from -6 to 6
- value_weight: float32 [2048, 1024], P('fs', 'tp'), may hold values from -0.125 to 0.125
- output_weight: float32 [1024, 2048], P('tp', 'fs'), may hold values from -0.1875 to 0.1875
- value_basis: bfloat16 [2048, 384], P('fs'), may hold values from -0.125 to 0.125
- output_basis: bfloat16 [2048, 384], P('fs'), may hold values from -0.125 to 0.125
- value_mean: float32 [384, 1024], P(None, 'tp'), may hold values from -4 to 4
- value_square: float32 [384, 1024], P(None, 'tp'), may hold values from 0.3 to 2
- output_mean: float32 [1024, 384], P('tp'), may hold values from -4 to 4
- output_square: float32 [1024, 384], P('tp'), may hold values from 0.3 to 2
Outputs:
- value_next: float32 [2048, 1024], P('fs', 'tp')
- value_copy: bfloat16 [2048, 1024], P(None, 'tp')
- value_step: float32 [2048, 1024], P('fs', 'tp')
- value_mean_next: float32 [384, 1024], P(None, 'tp')
- value_square_next: float32 [384, 1024], P(None, 'tp')
- output_next: float32 [1024, 2048], P('tp', 'fs')
- output_copy: bfloat16 [1024, 2048], P('tp')
- output_step: float32 [1024, 2048], P('tp', 'fs')
- output_mean_next: float32 [1024, 384], P('tp')
- output_square_next: float32 [1024, 384], P('tp')
The draws below stay inside these ranges and needn't reach their ends.
All inputs are finite; a program needn't handle non-finite values.
Results may differ from the reference program's by a relative error of at most 0.002.
Values may be sent and summed in bfloat16 or wider, within the bound.
A program may use at most 64 MiB of HBM per device.

```python
import math
import jax
import jax.numpy as jnp
from jax import lax

D = 2048
E = 1024
R = 384
TOKENS = 65536


def block_scale(own_key, dims, shards, smallest, high):
    loudness = 1.0
    for axis_at, parts in shards:
        draws = jax.random.uniform(jax.random.fold_in(jax.random.fold_in(own_key, 6), axis_at), (parts,), jnp.float32, smallest / len(shards), high / len(shards))
        loudness = loudness * jnp.repeat(jnp.exp(draws), dims[axis_at] // parts).reshape((-1,) + (1,) * (len(dims) - 1 - axis_at))
    return loudness


def normal_values(own_key, dims, spread, limit, pieces=(), kind=jnp.bfloat16):
    drawn = spread * jax.random.normal(own_key, dims, jnp.float32)
    if pieces:
        drawn = drawn * block_scale(own_key, dims, pieces, -0.22, 0.18)
    return jnp.clip(drawn, -limit, limit).astype(kind)


def setup_inputs(seed: int = 0) -> dict:
    keys = jax.random.split(jax.random.key(seed), 13)
    return {
        "block_input": normal_values(keys[0], (TOKENS, D), 1.0, 6.0, ((0, 64),)),
        "value_cotangent": normal_values(keys[1], (TOKENS, E), 1.0, 6.0, ((0, 64), (1, 8))),
        "mixed_output": normal_values(keys[2], (TOKENS, E), 1.0, 6.0, ((0, 64), (1, 8))),
        "output_cotangent": normal_values(keys[3], (TOKENS, D), 1.0, 6.0, ((0, 64),)),
        "value_weight": normal_values(keys[4], (D, E), D ** -0.5, 0.125, ((0, 64), (1, 8)), jnp.float32),
        "output_weight": normal_values(keys[5], (E, D), E ** -0.5, 0.1875, ((0, 8), (1, 64)), jnp.float32),
        "value_basis": normal_values(keys[6], (D, R), D ** -0.5, 0.125, ((0, 64),)),
        "output_basis": normal_values(keys[7], (D, R), D ** -0.5, 0.125, ((0, 64),)),
        "value_mean": normal_values(keys[8], (R, E), 0.7, 4.0, ((1, 8),), jnp.float32),
        "value_square": jnp.clip(jnp.exp(math.log(2.0) - 1.89712 * jax.random.uniform(keys[9], (R, E), jnp.float32) ** block_scale(keys[9], (R, E), ((1, 8),), -0.2, 0.2)), 0.3, 2.0),
        "output_mean": normal_values(keys[10], (E, R), 0.7, 4.0, ((0, 8),), jnp.float32),
        "output_square": jnp.clip(jnp.exp(math.log(2.0) - 1.89712 * jax.random.uniform(keys[11], (E, R), jnp.float32) ** block_scale(keys[11], (E, R), ((0, 8),), -0.2, 0.2)), 0.3, 2.0),
    }


def reference(block_input, value_cotangent, mixed_output, output_cotangent, value_weight, output_weight, value_basis, output_basis, value_mean, value_square, output_mean, output_square):
    highest = lax.Precision.HIGHEST
    scaling = 1.0 / math.sqrt(TOKENS)
    value_grad = jnp.dot(block_input.T, value_cotangent, preferred_element_type=jnp.float32)
    output_grad = jnp.dot(mixed_output.T, output_cotangent, preferred_element_type=jnp.float32)
    value_base = value_basis.astype(jnp.float32)
    output_base = output_basis.astype(jnp.float32)
    value_low = jnp.dot(value_base.T, value_grad, precision=highest) * scaling
    output_low = jnp.dot(output_grad, output_base, precision=highest) * scaling
    total_squares = jnp.sum(value_low * value_low) + jnp.sum(output_low * output_low)
    clip_scale = 1.0 / jnp.sqrt(1.0 + total_squares / (2.0 * R * E))
    value_scaled = clip_scale * value_low
    output_scaled = clip_scale * output_low
    value_mean_next = 0.8 * value_mean + 0.2 * value_scaled
    output_mean_next = 0.8 * output_mean + 0.2 * output_scaled
    value_square_next = 0.9 * value_square + 0.1 * value_scaled * value_scaled
    output_square_next = 0.9 * output_square + 0.1 * output_scaled * output_scaled
    value_norm = value_mean_next / jnp.sqrt(value_square_next + 0.1)
    output_norm = output_mean_next / jnp.sqrt(output_square_next + 0.1)
    value_step = jnp.dot(value_base, value_norm, precision=highest)
    output_step = jnp.dot(output_norm, output_base.T, precision=highest)
    value_next = value_weight - 0.02 * value_step
    output_next = output_weight - 0.02 * output_step
    return (value_next, value_next.astype(jnp.bfloat16), value_step, value_mean_next, value_square_next, output_next, output_next.astype(jnp.bfloat16), output_step, output_mean_next, output_square_next)
```

```python
import functools
import math

import jax
import jax.numpy as jnp
from jax import lax
from jax.experimental import pallas as pl
from jax.experimental.pallas import tpu as pltpu
from jax.sharding import PartitionSpec as P

NZ, NY, NX, NC = 16, 4, 4, 2
MESH = pl.DeviceIdType.MESH
W_BOUND = 0.1875
W_SLOPE = 250.0 / W_BOUND
CHUNKS = 4
FAR_FIRST = (8, 7, 9, 6, 10, 5, 11, 4, 12, 3, 13, 2, 14, 1, 15)


def coded(weight):
    size = jnp.exp2(jnp.abs(weight) * W_SLOPE - 125.0)
    return jnp.where(weight < 0, -size, size).astype(jnp.bfloat16)


def decoded(code):
    code = code.astype(jnp.float32)
    size = (jnp.log2(jnp.abs(code)) + 125.0) * (1.0 / W_SLOPE)
    return jnp.where(code < 0, -size, size)


def kernel(
    scaling,
    entries,
    x_hbm,
    v_hbm,
    m_hbm,
    oc_hbm,
    vb_hbm,
    ob_hbm,
    w_hbm,
    vmean_hbm,
    vsq_hbm,
    omean_hbm,
    osq_hbm,
    vmean_out,
    vsq_out,
    omean_out,
    osq_out,
    vcopy_out,
    ocopy_out,
    own_out,
    xs,
    ocs,
    vs,
    ms,
    shard,
    basis,
    weights,
    grads,
    ysend,
    yrecv,
    zsend,
    zrecv,
    lows,
    sums,
    small,
    vstate,
    ostate,
    load_sem,
    chunk_sem,
    bz_s,
    bz_r,
    by_s,
    by_r,
    bx_s,
    bx_r,
    bd_s,
    bd_r,
    ry_s,
    ry_r,
    rz_s,
    rz_r,
    az_s,
    az_r,
    ay_s,
    ay_r,
    cl_s,
    cl_r,
    wz_s,
    wz_r,
    wy_s,
    wy_r,
):
    fs, tp = lax.axis_index("fs"), lax.axis_index("tp")
    z, y = fs // NY, lax.rem(fs, NY)
    x, c = tp // NC, lax.rem(tp, NC)
    parity = lax.rem(x, 2)
    tokens, width = xs.shape
    rank = basis.shape[3]
    local = vs.shape[1]
    rows = basis.shape[2]

    def zdev(zz):
        return {"fs": zz * NY + y, "tp": tp}

    def ydev(yy):
        return {"fs": z * NY + yy, "tp": tp}

    def xdev(xx):
        return {"fs": fs, "tp": xx * NC + c}

    sibling = {"fs": fs, "tp": x * NC + 1 - c}

    def zup(j):
        return lax.rem(z + j, NZ)

    def yup(j):
        return lax.rem(y + j, NY)

    def xup(j):
        return lax.rem(x + j, NX)

    def remote(src, dst, ssem, rsem, device):
        return pltpu.make_async_remote_copy(
            src_ref=src, dst_ref=dst, send_sem=ssem, recv_sem=rsem, device_id=device, device_id_type=MESH
        )

    here = y * (NX * NC) + tp

    def plane(j):
        other = lax.rem(here + j, NY * NX * NC)
        return {"fs": z * NY + other // (NX * NC), "tp": lax.rem(other, NX * NC)}

    for k, far in enumerate((vb_hbm, ob_hbm)):

        @pl.when(c == k)
        def _(k=k, far=far):
            pltpu.make_async_copy(far, shard, load_sem.at[0]).start()

            @pl.when(parity == 0)
            def _():
                pltpu.make_async_copy(far, basis.at[k, fs], load_sem.at[1]).start()

    pltpu.make_async_copy(v_hbm, vs, load_sem.at[2]).start()
    pltpu.make_async_copy(m_hbm, ms, load_sem.at[3]).start()
    size = tokens // CHUNKS
    for t in range(CHUNKS):
        at = pl.ds(t * size, size)
        pltpu.make_async_copy(x_hbm.at[at], xs.at[at], chunk_sem.at[0, t]).start()
        pltpu.make_async_copy(oc_hbm.at[at], ocs.at[at], chunk_sem.at[1, t]).start()
    pltpu.make_async_copy(vmean_hbm, vstate.at[0], load_sem.at[4]).start()
    pltpu.make_async_copy(vsq_hbm, vstate.at[1], load_sem.at[5]).start()
    pltpu.make_async_copy(omean_hbm, ostate.at[0], load_sem.at[6]).start()
    pltpu.make_async_copy(osq_hbm, ostate.at[1], load_sem.at[7]).start()
    pltpu.make_async_copy(w_hbm, weights.at[fs], load_sem.at[8]).start()

    barrier = pltpu.get_barrier_semaphore()
    for j in range(1, NZ):
        pl.semaphore_signal(barrier, inc=1, device_id=zdev(zup(j)), device_id_type=MESH)
    for j in range(1, NY * NX * NC):
        pl.semaphore_signal(barrier, inc=1, device_id=plane(j), device_id_type=MESH)

    pltpu.make_async_copy(v_hbm, vs, load_sem.at[2]).wait()
    pltpu.make_async_copy(m_hbm, ms, load_sem.at[3]).wait()
    across = (((0,), (0,)), ((), ()))
    for t in range(CHUNKS):
        at = pl.ds(t * size, size)
        for k, (far, near, thin) in enumerate(((x_hbm, xs, vs), (oc_hbm, ocs, ms))):
            pltpu.make_async_copy(far.at[at], near.at[at], chunk_sem.at[k, t]).wait()
            part = lax.dot_general(thin[at, :], near[at, :], across, preferred_element_type=jnp.float32)
            if t == 0:
                grads[k] = part
            else:
                grads[k] += part

    pltpu.make_async_copy(vb_hbm, shard, load_sem.at[0]).wait()

    @pl.when(parity == 0)
    def _():
        pltpu.make_async_copy(vb_hbm, basis.at[c, fs], load_sem.at[1]).wait()

    pltpu.make_async_copy(w_hbm, weights.at[fs], load_sem.at[8]).wait()
    pl.semaphore_wait(barrier, NZ - 1 + NY * NX * NC - 1)

    def offset(n, p):
        odd = lax.rem(n + p, 2)
        return (n + 1) * odd - n * (1 - odd)

    def from_z(n, p):
        return lax.rem(z - offset(n, p) + NZ, NZ)

    def bz(n):
        to = lax.rem(z + offset(n, parity) + NZ, NZ)
        return remote(shard, basis.at[c, fs], bz_s.at[n], bz_r.at[n], zdev(to))

    def bz_recv(n):
        block = basis.at[c, from_z(n, parity) * NY + y]
        return remote(block, block, bz_s.at[n], bz_r.at[n], zdev(zup(1)))

    def by(n, j):
        block = basis.at[c, from_z(n, parity) * NY + y]
        return remote(block, block, by_s.at[n, j - 1], by_r.at[n, j - 1], ydev(yup(j)))

    def by_recv(n, j):
        block = basis.at[c, from_z(n, parity) * NY + yup(NY - j)]
        return remote(block, block, by_s.at[n, j - 1], by_r.at[n, j - 1], ydev(yup(1)))

    half = NY // 2

    def bx(n, d):
        block = basis.at[c, pl.ds(from_z(n, parity) * NY + d * half, half)]
        return remote(block, block, bx_s.at[n, d], bx_r.at[n, d], xdev(xup(1 if d == 0 else NX - 1)))

    def bx_recv(n, d):
        block = basis.at[c, pl.ds(from_z(n, 1 - parity) * NY + d * half, half)]
        return remote(block, block, bx_s.at[n, d], bx_r.at[n, d], xdev(xup(1)))

    def bd(n, w):
        block = basis.at[c, pl.ds(from_z(n, parity if w == 0 else 1 - parity) * NY, NY)]
        return remote(block, block, bd_s.at[n, w], bd_r.at[n, w], sibling)

    def bd_recv(n, w):
        block = basis.at[1 - c, pl.ds(from_z(n, parity if w == 0 else 1 - parity) * NY, NY)]
        return remote(block, block, bd_s.at[n, w], bd_r.at[n, w], sibling)

    steps = NZ // 2

    def when_odd(n, act):
        if n == 0:
            pl.when(parity == 1)(act)
        else:
            act()

    for n in range(steps):
        when_odd(n, lambda n=n: bz(n).start())

    def wz(j):
        block = weights.at[fs]
        return remote(block, block, wz_s.at[j - 1], wz_r.at[j - 1], zdev(zup(j)))

    def wz_recv(j):
        block = weights.at[zup(NZ - j) * NY + y]
        return remote(block, block, wz_s.at[j - 1], wz_r.at[j - 1], zdev(zup(1)))

    def wy(i, j):
        block = weights.at[i * NY + y]
        return remote(block, block, wy_s.at[i, j - 1], wy_r.at[i, j - 1], ydev(yup(j)))

    def wy_recv(i, j):
        block = weights.at[i * NY + yup(NY - j)]
        return remote(block, block, wy_s.at[i, j - 1], wy_r.at[i, j - 1], ydev(yup(1)))

    for j in FAR_FIRST:
        wz(j).start()

    lag_y, lag_x = 2, 4
    for s in range(steps + lag_x):
        if s < steps:
            when_odd(s, lambda s=s: bz_recv(s).wait_recv())
            for j in range(1, NY):
                by(s, j).start()
        n = s - lag_y
        if 0 <= n < steps:
            for j in range(1, NY):
                by_recv(n, j).wait_recv()
            bx(n, 0).start()
            bx(n, 1).start()
            bd(n, 0).start()
        n = s - lag_x
        if 0 <= n < steps:
            bx_recv(n, 0).wait_recv()
            bx_recv(n, 1).wait_recv()
            bd(n, 1).start()

    for n in range(steps):
        for w in range(2):
            bd_recv(n, w).wait_recv()

    quarter = local // NY
    for k in range(2):
        whole = grads[k]
        high = whole.astype(jnp.bfloat16)
        low = (whole - high.astype(jnp.float32)).astype(jnp.bfloat16)
        base = basis[k].reshape(-1, rank)
        part = jnp.dot(high, base, preferred_element_type=jnp.float32) + jnp.dot(
            low, base, preferred_element_type=jnp.float32
        )
        ysend[k] = (part * scaling).reshape(NY, quarter, rank)
        for j in (2, 1, 3):
            remote(
                ysend.at[k, yup(j)], yrecv.at[k, j - 1], ry_s.at[k, j - 1], ry_r.at[k, j - 1], ydev(yup(j))
            ).start()

    for j in FAR_FIRST:
        wz_recv(j).wait_recv()
    for i in range(NZ):
        for j in range(1, NY):
            wy(i, j).start()

    def ry_recv(k, j):
        return remote(ysend.at[k, 0], yrecv.at[k, j - 1], ry_s.at[k, j - 1], ry_r.at[k, j - 1], ydev(yup(j)))

    piece = 2 * quarter // NZ
    for k in range(2):
        for j in range(1, NY):
            ry_recv(k, j).wait_recv()
        total = (ysend[k, y] + yrecv[k, 0]) + (yrecv[k, 1] + yrecv[k, 2])
        for i in range(NZ // 2):
            zsend[k * (NZ // 2) + i] = total[i * piece : (i + 1) * piece]

    def rz(j):
        return remote(zsend.at[zup(j)], zrecv.at[j - 1], rz_s.at[j - 1], rz_r.at[j - 1], zdev(zup(j)))

    for j in FAR_FIRST:
        rz(j).start()
    total = zsend[z]
    for j in reversed(FAR_FIRST):
        rz(j).wait_recv()
        total = total + zrecv[j - 1]
    lows[y, z] = total.astype(jnp.bfloat16)

    def az(j):
        block = lows.at[y, z]
        return remote(block, block, az_s.at[j - 1], az_r.at[j - 1], zdev(zup(j)))

    def az_recv(j):
        block = lows.at[y, zup(NZ - j)]
        return remote(block, block, az_s.at[j - 1], az_r.at[j - 1], zdev(zup(1)))

    for j in FAR_FIRST:
        az(j).start()
    for j in reversed(FAR_FIRST):
        az_recv(j).wait_recv()

    def ay(j):
        block = lows.at[y]
        return remote(block, block, ay_s.at[j - 1], ay_r.at[j - 1], ydev(yup(j)))

    def ay_recv(j):
        block = lows.at[yup(NY - j)]
        return remote(block, block, ay_s.at[j - 1], ay_r.at[j - 1], ydev(yup(1)))

    for j in (2, 1, 3):
        ay(j).start()

    mine = lows[y].astype(jnp.float32)
    square = jnp.sum(mine * mine)
    sums[here] = jnp.full((1, 128), square, jnp.float32)

    def cl(j):
        block = sums.at[here]
        return remote(block, block, cl_s.at[j - 1], cl_r.at[j - 1], plane(j))

    def cl_recv(j):
        block = sums.at[lax.rem(here + NY * NX * NC - j, NY * NX * NC)]
        return remote(block, block, cl_s.at[j - 1], cl_r.at[j - 1], plane(1))

    for j in range(1, NY * NX * NC):
        cl(j).start()
    for j in (1, 3, 2):
        ay_recv(j).wait_recv()
    for k in range(2):
        for yy in range(NY):
            for i in range(NZ // 2):
                at = yy * quarter + i * piece
                small[k, at : at + piece, :] = lows[yy, k * (NZ // 2) + i].astype(jnp.float32)
    for j in range(1, NY * NX * NC):
        cl_recv(j).wait_recv()
    everyone = jnp.sum(sums[...], axis=0)
    clip = 1.0 / jnp.sqrt(1.0 + everyone[:, 0:1] / entries)

    for i, (far, near) in enumerate(
        (
            (vmean_hbm, vstate.at[0]),
            (vsq_hbm, vstate.at[1]),
            (omean_hbm, ostate.at[0]),
            (osq_hbm, ostate.at[1]),
        )
    ):
        pltpu.make_async_copy(far, near, load_sem.at[4 + i]).wait()

    def advance(low, state, mean_out, sq_out):
        scaled = low * clip
        mean = 0.8 * state[0] + 0.2 * scaled
        sq = 0.9 * state[1] + 0.1 * scaled * scaled
        mean_out[...] = mean
        sq_out[...] = sq
        return mean / jnp.sqrt(sq + 0.1)

    norms = (
        advance(small[0].T, vstate, vmean_out, vsq_out),
        advance(small[1], ostate, omean_out, osq_out).T,
    )
    for i in range(NZ):
        for j in range(1, NY):
            wy_recv(i, j).wait_recv()
    copies = (vcopy_out, ocopy_out)
    block_rows = 256
    per = block_rows // rows
    for k in range(2):
        high = norms[k].astype(jnp.bfloat16)
        low = (norms[k] - high.astype(jnp.float32)).astype(jnp.bfloat16)
        both = jnp.concatenate([high, low], axis=1)
        for b in range(width // block_rows):
            base = basis[k, b * per : (b + 1) * per].reshape(block_rows, rank)
            step = jnp.dot(base, both, preferred_element_type=jnp.float32)
            step = step[:, :local] + step[:, local:]
            weight = decoded(weights[b * per : (b + 1) * per, k].reshape(block_rows, local))
            copies[k][b * block_rows : (b + 1) * block_rows, :] = (weight - 0.02 * step).astype(jnp.bfloat16)
        step = jnp.dot(basis[k, fs], both, preferred_element_type=jnp.float32)
        own_out[k] = step[:, :local] + step[:, local:]

    for i in range(NZ):
        for j in range(1, NY):
            wy(i, j).wait_send()
    for n in range(steps):
        when_odd(n, lambda n=n: bz(n).wait_send())
        for j in range(1, NY):
            by(n, j).wait_send()
        for w in range(2):
            bx(n, w).wait_send()
            bd(n, w).wait_send()
    for j in range(1, NZ):
        wz(j).wait_send()
        rz(j).wait_send()
        az(j).wait_send()
    for j in range(1, NY):
        ay(j).wait_send()
        for k in range(2):
            ry_recv(k, j).wait_send()
    for j in range(1, NY * NX * NC):
        cl(j).wait_send()


def on_device(
    block_input,
    value_cotangent,
    mixed_output,
    output_cotangent,
    value_weight,
    output_weight,
    value_basis,
    output_basis,
    value_mean,
    value_square,
    output_mean,
    output_square,
):
    tokens, width = block_input.shape
    local = value_cotangent.shape[1]
    rows, rank = value_basis.shape
    devices = lax.axis_size("fs")
    scaling = 1.0 / math.sqrt(tokens * devices)
    entries = 2.0 * rank * local * lax.axis_size("tp")
    quarter = local // NY
    piece = 2 * quarter // NZ
    f32, bf16 = jnp.float32, jnp.bfloat16
    sent = coded(jnp.stack([value_weight, output_weight.T]))
    hbm = pl.BlockSpec(memory_space=pl.ANY)
    vmem = pl.BlockSpec(memory_space=pltpu.VMEM)
    dma = pltpu.SemaphoreType.DMA
    near = NY * NX * NC - 1
    out = pl.pallas_call(
        functools.partial(kernel, scaling, entries),
        out_shape=(
            jax.ShapeDtypeStruct((rank, local), f32),
            jax.ShapeDtypeStruct((rank, local), f32),
            jax.ShapeDtypeStruct((local, rank), f32),
            jax.ShapeDtypeStruct((local, rank), f32),
            jax.ShapeDtypeStruct((width, local), bf16),
            jax.ShapeDtypeStruct((width, local), bf16),
            jax.ShapeDtypeStruct((2, rows, local), f32),
        ),
        in_specs=[hbm] * 11,
        out_specs=(vmem,) * 7,
        scratch_shapes=[
            pltpu.VMEM((tokens, width), bf16),
            pltpu.VMEM((tokens, width), bf16),
            pltpu.VMEM((tokens, local), bf16),
            pltpu.VMEM((tokens, local), bf16),
            pltpu.VMEM((rows, rank), bf16),
            pltpu.VMEM((2, devices, rows, rank), bf16),
            pltpu.VMEM((devices, 2, rows, local), bf16),
            pltpu.VMEM((2, local, width), f32),
            pltpu.VMEM((2, NY, quarter, rank), f32),
            pltpu.VMEM((2, NY - 1, quarter, rank), f32),
            pltpu.VMEM((NZ, piece, rank), f32),
            pltpu.VMEM((NZ - 1, piece, rank), f32),
            pltpu.VMEM((NY, NZ, piece, rank), bf16),
            pltpu.VMEM((NY * NX * NC, 1, 128), f32),
            pltpu.VMEM((2, local, rank), f32),
            pltpu.VMEM((2, rank, local), f32),
            pltpu.VMEM((2, local, rank), f32),
            dma((9,)),
            dma((2, CHUNKS)),
            dma((NZ // 2,)),
            dma((NZ // 2,)),
            dma((NZ // 2, NY - 1)),
            dma((NZ // 2, NY - 1)),
            dma((NZ // 2, 2)),
            dma((NZ // 2, 2)),
            dma((NZ // 2, 2)),
            dma((NZ // 2, 2)),
            dma((2, NY - 1)),
            dma((2, NY - 1)),
            dma((NZ - 1,)),
            dma((NZ - 1,)),
            dma((NZ - 1,)),
            dma((NZ - 1,)),
            dma((NY - 1,)),
            dma((NY - 1,)),
            dma((near,)),
            dma((near,)),
            dma((NZ - 1,)),
            dma((NZ - 1,)),
            dma((NZ, NY - 1)),
            dma((NZ, NY - 1)),
        ],
        compiler_params=pltpu.CompilerParams(
            collective_id=0, has_side_effects=True, vmem_limit_bytes=60 * 1024 * 1024
        ),
    )(
        block_input,
        value_cotangent,
        mixed_output,
        output_cotangent,
        value_basis,
        output_basis,
        sent,
        value_mean,
        value_square,
        output_mean,
        output_square,
    )
    value_mean_next, value_square_next, output_mean_next, output_square_next, value_copy, turned, own = out
    output_copy = turned.T
    value_step = own[0]
    output_step = own[1].T
    value_next = value_weight - 0.02 * value_step
    output_next = output_weight - 0.02 * output_step
    return (
        value_next,
        value_copy,
        value_step,
        value_mean_next,
        value_square_next,
        output_next,
        output_copy,
        output_step,
        output_mean_next,
        output_square_next,
    )


def solution(mesh):
    return jax.shard_map(
        on_device,
        mesh=mesh,
        in_specs=(
            P("fs", None),
            P("fs", "tp"),
            P("fs", "tp"),
            P("fs", None),
            P("fs", "tp"),
            P("tp", "fs"),
            P("fs", None),
            P("fs", None),
            P(None, "tp"),
            P(None, "tp"),
            P("tp", None),
            P("tp", None),
        ),
        out_specs=(
            P("fs", "tp"),
            P(None, "tp"),
            P("fs", "tp"),
            P(None, "tp"),
            P(None, "tp"),
            P("tp", "fs"),
            P("tp", None),
            P("tp", "fs"),
            P("tp", None),
            P("tp", None),
        ),
        check_vma=False,
    )
```

```python
import functools
import math

import jax
import jax.numpy as jnp
from jax import lax
from jax.experimental import pallas as pl
from jax.experimental.pallas import tpu as pltpu
from jax.sharding import PartitionSpec as P

NZ, NY, NX, NC = 16, 4, 4, 2
MESH = pl.DeviceIdType.MESH
W_BOUND = 0.1875
W_SLOPE = 250.0 / W_BOUND
CHUNKS = 4
NEAR = (4, 12, 3, 13, 2, 14, 1, 15)
IN_ORDER = (0, 1, 15, 2, 14, 3, 13, 4, 12, 5, 11, 6, 10, 7, 9, 8)
RELAYED = {4: (4, 3, 2, 1), 12: (-3, -2, -1)}
LAG_Y, LAG_X = 5, 9
FAR_FIRST = (8, 7, 9, 6, 10, 5, 11, 4, 12, 3, 13, 2, 14, 1, 15)


def coded(weight):
    size = jnp.exp2(jnp.abs(weight) * W_SLOPE - 125.0)
    return jnp.where(weight < 0, -size, size).astype(jnp.bfloat16)


def decoded(code):
    code = code.astype(jnp.float32)
    size = (jnp.log2(jnp.abs(code)) + 125.0) * (1.0 / W_SLOPE)
    return jnp.where(code < 0, -size, size)


def kernel(
    scaling,
    entries,
    x_hbm,
    v_hbm,
    m_hbm,
    oc_hbm,
    vb_hbm,
    ob_hbm,
    vw_hbm,
    ow_hbm,
    vmean_hbm,
    vsq_hbm,
    omean_hbm,
    osq_hbm,
    vnext_out,
    vcopy_out,
    vstep_out,
    vmean_out,
    vsq_out,
    onext_out,
    ocopy_out,
    ostep_out,
    omean_out,
    osq_out,
    xs,
    ocs,
    vs,
    ms,
    basis,
    owned,
    weights,
    grads,
    ysend,
    yrecv,
    zsend,
    zrecv,
    lows,
    sums,
    small,
    vstate,
    ostate,
    load_sem,
    chunk_sem,
    bz_s,
    bz_r,
    by_s,
    by_r,
    bx_s,
    bx_r,
    bd_s,
    bd_r,
    ry_s,
    ry_r,
    rz_s,
    rz_r,
    az_s,
    az_r,
    ay_s,
    ay_r,
    cl_s,
    cl_r,
    wz_s,
    wz_r,
    wy_s,
    wy_r,
):
    fs, tp = lax.axis_index("fs"), lax.axis_index("tp")
    z, y = fs // NY, lax.rem(fs, NY)
    x, c = tp // NC, lax.rem(tp, NC)
    parity = lax.rem(x, 2)
    tokens, width = xs.shape
    rank = basis.shape[3]
    local = vs.shape[1]
    rows = basis.shape[2]

    def zdev(zz):
        return {"fs": zz * NY + y, "tp": tp}

    def ydev(yy):
        return {"fs": z * NY + yy, "tp": tp}

    def xdev(xx):
        return {"fs": fs, "tp": xx * NC + c}

    sibling = {"fs": fs, "tp": x * NC + 1 - c}

    def zup(j):
        return lax.rem(z + j, NZ)

    def yup(j):
        return lax.rem(y + j, NY)

    def xup(j):
        return lax.rem(x + j, NX)

    pending = []

    def go(copy):
        copy.start()
        pending.append(copy)

    def remote(src, dst, ssem, rsem, device):
        return pltpu.make_async_remote_copy(
            src_ref=src, dst_ref=dst, send_sem=ssem, recv_sem=rsem, device_id=device, device_id_type=MESH
        )

    here = y * (NX * NC) + tp

    def plane(j):
        other = lax.rem(here + j, NY * NX * NC)
        return {"fs": z * NY + other // (NX * NC), "tp": lax.rem(other, NX * NC)}

    half = rows // 2

    def part_of(p):
        return pl.ds(pl.multiple_of(p * half, half), half)

    for k, far in enumerate((vb_hbm, ob_hbm)):

        @pl.when(c == k)
        def _(k=k, far=far):
            pltpu.make_async_copy(far.at[part_of(parity)], basis.at[k, fs, part_of(parity)], load_sem.at[0]).start()

    pltpu.make_async_copy(vw_hbm, owned.at[0], load_sem.at[1]).start()
    pltpu.make_async_copy(ow_hbm, owned.at[1], load_sem.at[8]).start()
    pltpu.make_async_copy(v_hbm, vs, load_sem.at[2]).start()
    pltpu.make_async_copy(m_hbm, ms, load_sem.at[3]).start()
    size = tokens // CHUNKS
    for t in range(CHUNKS):
        at = pl.ds(t * size, size)
        pltpu.make_async_copy(x_hbm.at[at], xs.at[at], chunk_sem.at[0, t]).start()
        pltpu.make_async_copy(oc_hbm.at[at], ocs.at[at], chunk_sem.at[1, t]).start()
    pltpu.make_async_copy(vmean_hbm, vstate.at[0], load_sem.at[4]).start()
    pltpu.make_async_copy(vsq_hbm, vstate.at[1], load_sem.at[5]).start()
    pltpu.make_async_copy(omean_hbm, ostate.at[0], load_sem.at[6]).start()
    pltpu.make_async_copy(osq_hbm, ostate.at[1], load_sem.at[7]).start()

    barrier = pltpu.get_barrier_semaphore()
    for j in NEAR:
        pl.semaphore_signal(barrier, inc=1, device_id=zdev(zup(j)), device_id_type=MESH)
    for j in range(1, NY * NX * NC):
        pl.semaphore_signal(barrier, inc=1, device_id=plane(j), device_id_type=MESH)

    pltpu.make_async_copy(vb_hbm.at[part_of(0)], basis.at[c, fs, part_of(parity)], load_sem.at[0]).wait()
    pltpu.make_async_copy(vw_hbm, owned.at[0], load_sem.at[1]).wait()
    pltpu.make_async_copy(ow_hbm, owned.at[1], load_sem.at[8]).wait()
    weights[fs] = coded(owned[...])

    pltpu.make_async_copy(v_hbm, vs, load_sem.at[2]).wait()
    pltpu.make_async_copy(m_hbm, ms, load_sem.at[3]).wait()
    across = (((0,), (0,)), ((), ()))
    for t in range(CHUNKS):
        at = pl.ds(t * size, size)
        for k, (far, near, thin) in enumerate(((x_hbm, xs, vs), (oc_hbm, ocs, ms))):
            pltpu.make_async_copy(far.at[at], near.at[at], chunk_sem.at[k, t]).wait()
            part = lax.dot_general(thin[at, :], near[at, :], across, preferred_element_type=jnp.float32)
            if t == 0:
                grads[k] = part
            else:
                grads[k] += part

    pl.semaphore_wait(barrier, len(NEAR) + NY * NX * NC - 1)

    def relay(block_of, ssem, rsem):
        def down(d, to):
            block = block_of(zup(NZ - d if d else 0))
            at = (d + to) % NZ - 1
            return remote(block, block, ssem.at[at], rsem.at[at], zdev(zup(to % NZ)))

        def arrived(d):
            block = block_of(zup(NZ - d))
            remote(block, block, ssem.at[d - 1], rsem.at[d - 1], zdev(zup(1))).wait_recv()

        return down, arrived

    def basis_row(zz):
        return basis.at[c, zz * NY + y, part_of(parity)]

    def weight_row(zz):
        return weights.at[zz * NY + y]

    send_basis, basis_came = relay(basis_row, bz_s, bz_r)
    send_weight, weight_came = relay(weight_row, wz_s, wz_r)

    def by(d, j):
        block = basis_row(zup(NZ - d if d else 0))
        return remote(block, block, by_s.at[d, j - 1], by_r.at[d, j - 1], ydev(yup(j)))

    def by_recv(d, j):
        block = basis.at[c, zup(NZ - d if d else 0) * NY + yup(NY - j), part_of(parity)]
        return remote(block, block, by_s.at[d, j - 1], by_r.at[d, j - 1], ydev(yup(1)))

    pair = NY // 2

    def bx(d, w):
        block = basis.at[c, pl.ds(zup(NZ - d if d else 0) * NY + w * pair, pair), part_of(parity)]
        return remote(block, block, bx_s.at[d, w], bx_r.at[d, w], xdev(xup(1 if w == 0 else NX - 1)))

    def bx_recv(d, w):
        block = basis.at[c, pl.ds(zup(NZ - d if d else 0) * NY + w * pair, pair), part_of(1 - parity)]
        return remote(block, block, bx_s.at[d, w], bx_r.at[d, w], xdev(xup(1)))

    def bd(d, w):
        block = basis.at[c, pl.ds(zup(NZ - d if d else 0) * NY, NY), part_of(parity if w == 0 else 1 - parity)]
        return remote(block, block, bd_s.at[d, w], bd_r.at[d, w], sibling)

    def bd_recv(d, w):
        block = basis.at[1 - c, pl.ds(zup(NZ - d if d else 0) * NY, NY), part_of(parity if w == 0 else 1 - parity)]
        return remote(block, block, bd_s.at[d, w], bd_r.at[d, w], sibling)

    for to in NEAR:
        go(send_basis(0, to))
    for s in range(NZ + LAG_X):
        if s < NZ:
            d = IN_ORDER[s]
            if d:
                basis_came(d)
            if d in RELAYED:
                for to in RELAYED[d]:
                    go(send_basis(d, to))
            for j in (2, 1, 3):
                go(by(d, j))
        if 0 <= s - LAG_Y < NZ:
            d = IN_ORDER[s - LAG_Y]
            for j in range(1, NY):
                by_recv(d, j).wait_recv()
            for w in range(2):
                go(bx(d, w))
            go(bd(d, 0))
        if s == NZ:
            for to in NEAR:
                go(send_weight(0, to))
        if 0 <= s - LAG_X < NZ:
            d = IN_ORDER[s - LAG_X]
            for w in range(2):
                bx_recv(d, w).wait_recv()
            go(bd(d, 1))

    def wy(d, j):
        block = weight_row(zup(NZ - d if d else 0))
        return remote(block, block, wy_s.at[d, j - 1], wy_r.at[d, j - 1], ydev(yup(j)))

    def wy_recv(d, j):
        block = weights.at[zup(NZ - d if d else 0) * NY + yup(NY - j)]
        return remote(block, block, wy_s.at[d, j - 1], wy_r.at[d, j - 1], ydev(yup(1)))

    for d in IN_ORDER:
        for w in range(2):
            bd_recv(d, w).wait_recv()

    quarter = local // NY
    for k in range(2):
        whole = grads[k]
        high = whole.astype(jnp.bfloat16)
        low = (whole - high.astype(jnp.float32)).astype(jnp.bfloat16)
        base = basis[k].reshape(-1, rank)
        part = jnp.dot(high, base, preferred_element_type=jnp.float32) + jnp.dot(
            low, base, preferred_element_type=jnp.float32
        )
        ysend[k] = (part * scaling).reshape(NY, quarter, rank)
        for j in (2, 1, 3):
            go(
                remote(
                    ysend.at[k, yup(j)], yrecv.at[k, j - 1], ry_s.at[k, j - 1], ry_r.at[k, j - 1], ydev(yup(j))
                )
            )

    for d in IN_ORDER[1:9]:
        weight_came(d)
        for to in RELAYED.get(d, ()):
            go(send_weight(d, to))

    def ry_recv(k, j):
        return remote(ysend.at[k, 0], yrecv.at[k, j - 1], ry_s.at[k, j - 1], ry_r.at[k, j - 1], ydev(yup(j)))

    piece = 2 * quarter // NZ
    for k in range(2):
        for j in range(1, NY):
            ry_recv(k, j).wait_recv()
        total = (ysend[k, y] + yrecv[k, 0]) + (yrecv[k, 1] + yrecv[k, 2])
        for i in range(NZ // 2):
            zsend[k * (NZ // 2) + i] = total[i * piece : (i + 1) * piece]

    def rz(j):
        return remote(zsend.at[zup(j)], zrecv.at[j - 1], rz_s.at[j - 1], rz_r.at[j - 1], zdev(zup(j)))

    for j in FAR_FIRST:
        go(rz(j))
    for d in IN_ORDER[:9]:
        for j in (2, 1, 3):
            go(wy(d, j))
    total = zsend[z]
    for j in reversed(FAR_FIRST):
        rz(j).wait_recv()
        total = total + zrecv[j - 1]
    lows[y, z] = total.astype(jnp.bfloat16)

    def az(j):
        block = lows.at[y, z]
        return remote(block, block, az_s.at[j - 1], az_r.at[j - 1], zdev(zup(j)))

    def az_recv(j):
        block = lows.at[y, zup(NZ - j)]
        return remote(block, block, az_s.at[j - 1], az_r.at[j - 1], zdev(zup(1)))

    for j in FAR_FIRST:
        go(az(j))
    for d in IN_ORDER[9:]:
        weight_came(d)
        for j in (2, 1, 3):
            go(wy(d, j))
    for j in reversed(FAR_FIRST):
        az_recv(j).wait_recv()

    def ay(j):
        block = lows.at[y]
        return remote(block, block, ay_s.at[j - 1], ay_r.at[j - 1], ydev(yup(j)))

    def ay_recv(j):
        block = lows.at[yup(NY - j)]
        return remote(block, block, ay_s.at[j - 1], ay_r.at[j - 1], ydev(yup(1)))

    for j in (2, 1, 3):
        go(ay(j))

    mine = lows[y].astype(jnp.float32)
    square = jnp.sum(mine * mine)
    sums[here] = jnp.full((1, 128), square, jnp.float32)

    def cl(j):
        block = sums.at[here]
        return remote(block, block, cl_s.at[j - 1], cl_r.at[j - 1], plane(j))

    def cl_recv(j):
        block = sums.at[lax.rem(here + NY * NX * NC - j, NY * NX * NC)]
        return remote(block, block, cl_s.at[j - 1], cl_r.at[j - 1], plane(1))

    for j in range(1, NY * NX * NC):
        go(cl(j))
    for j in (1, 3, 2):
        ay_recv(j).wait_recv()
    for k in range(2):
        for yy in range(NY):
            for i in range(NZ // 2):
                at = yy * quarter + i * piece
                small[k, at : at + piece, :] = lows[yy, k * (NZ // 2) + i].astype(jnp.float32)
    for j in range(1, NY * NX * NC):
        cl_recv(j).wait_recv()
    everyone = jnp.sum(sums[...], axis=0)
    clip = 1.0 / jnp.sqrt(1.0 + everyone[:, 0:1] / entries)

    for i, (far, near) in enumerate(
        (
            (vmean_hbm, vstate.at[0]),
            (vsq_hbm, vstate.at[1]),
            (omean_hbm, ostate.at[0]),
            (osq_hbm, ostate.at[1]),
        )
    ):
        pltpu.make_async_copy(far, near, load_sem.at[4 + i]).wait()

    def advance(low, state, mean_out, sq_out):
        scaled = low * clip
        mean = 0.8 * state[0] + 0.2 * scaled
        sq = 0.9 * state[1] + 0.1 * scaled * scaled
        mean_out[...] = mean
        sq_out[...] = sq
        return mean / jnp.sqrt(sq + 0.1)

    norms = (
        advance(small[0].T, vstate, vmean_out, vsq_out),
        advance(small[1], ostate, omean_out, osq_out).T,
    )
    for d in IN_ORDER:
        for j in range(1, NY):
            wy_recv(d, j).wait_recv()
    block_rows = 256
    per = block_rows // rows
    for k in range(2):
        high = norms[k].astype(jnp.bfloat16)
        low = (norms[k] - high.astype(jnp.float32)).astype(jnp.bfloat16)
        both = jnp.concatenate([high, low], axis=1)
        for b in range(width // block_rows):
            base = basis[k, b * per : (b + 1) * per].reshape(block_rows, rank)
            step = jnp.dot(base, both, preferred_element_type=jnp.float32)
            step = step[:, :local] + step[:, local:]
            weight = decoded(weights[b * per : (b + 1) * per, k].reshape(block_rows, local))
            moved = weight - 0.02 * step
            at = slice(b * block_rows, (b + 1) * block_rows)
            if k == 0:
                vcopy_out[at, :] = moved.astype(jnp.bfloat16)
            else:
                ocopy_out[:, at] = moved.T.astype(jnp.bfloat16)
        step = jnp.dot(basis[k, fs], both, preferred_element_type=jnp.float32)
        step = step[:, :local] + step[:, local:]
        (vstep_out, ostep_out)[k][...] = step
        (vnext_out, onext_out)[k][...] = owned[k] - 0.02 * step

    for copy in pending:
        copy.wait_send()


def store(*refs):
    count = len(refs) // 2
    for near, far in zip(refs[:count], refs[count:]):
        far[...] = near[...]


def on_device(
    block_input,
    value_cotangent,
    mixed_output,
    output_cotangent,
    value_weight,
    output_weight,
    value_basis,
    output_basis,
    value_mean,
    value_square,
    output_mean,
    output_square,
):
    tokens, width = block_input.shape
    local = value_cotangent.shape[1]
    rows, rank = value_basis.shape
    devices = lax.axis_size("fs")
    scaling = 1.0 / math.sqrt(tokens * devices)
    entries = 2.0 * rank * local * lax.axis_size("tp")
    quarter = local // NY
    piece = 2 * quarter // NZ
    f32, bf16 = jnp.float32, jnp.bfloat16
    hbm = pl.BlockSpec(memory_space=pltpu.HBM)
    vmem = pl.BlockSpec(memory_space=pltpu.VMEM)
    dma = pltpu.SemaphoreType.DMA
    near = NY * NX * NC - 1
    shapes = (
        jax.ShapeDtypeStruct((rows, local), f32),
        jax.ShapeDtypeStruct((width, local), bf16),
        jax.ShapeDtypeStruct((rows, local), f32),
        jax.ShapeDtypeStruct((rank, local), f32),
        jax.ShapeDtypeStruct((rank, local), f32),
        jax.ShapeDtypeStruct((rows, local), f32),
        jax.ShapeDtypeStruct((local, width), bf16),
        jax.ShapeDtypeStruct((rows, local), f32),
        jax.ShapeDtypeStruct((local, rank), f32),
        jax.ShapeDtypeStruct((local, rank), f32),
    )
    out = pl.pallas_call(
        functools.partial(kernel, scaling, entries),
        out_shape=shapes,
        in_specs=[hbm] * 12,
        out_specs=(vmem,) * len(shapes),
        scratch_shapes=[
            pltpu.VMEM((tokens, width), bf16),
            pltpu.VMEM((tokens, width), bf16),
            pltpu.VMEM((tokens, local), bf16),
            pltpu.VMEM((tokens, local), bf16),
            pltpu.VMEM((2, devices, rows, rank), bf16),
            pltpu.VMEM((2, rows, local), f32),
            pltpu.VMEM((devices, 2, rows, local), bf16),
            pltpu.VMEM((2, local, width), f32),
            pltpu.VMEM((2, NY, quarter, rank), f32),
            pltpu.VMEM((2, NY - 1, quarter, rank), f32),
            pltpu.VMEM((NZ, piece, rank), f32),
            pltpu.VMEM((NZ - 1, piece, rank), f32),
            pltpu.VMEM((NY, NZ, piece, rank), bf16),
            pltpu.VMEM((NY * NX * NC, 1, 128), f32),
            pltpu.VMEM((2, local, rank), f32),
            pltpu.VMEM((2, rank, local), f32),
            pltpu.VMEM((2, local, rank), f32),
            dma((9,)),
            dma((2, CHUNKS)),
            *[dma((NZ - 1,))] * 2,
            *[dma((NZ, NY - 1))] * 2,
            *[dma((NZ, 2))] * 4,
            *[dma((2, NY - 1))] * 2,
            *[dma((NZ - 1,))] * 4,
            *[dma((NY - 1,))] * 2,
            *[dma((near,))] * 2,
            *[dma((NZ - 1,))] * 2,
            *[dma((NZ, NY - 1))] * 2,
        ],
        compiler_params=pltpu.CompilerParams(
            collective_id=0, has_side_effects=True, vmem_limit_bytes=32 * 1024 * 1024
        ),
    )(
        block_input,
        value_cotangent,
        mixed_output,
        output_cotangent,
        value_basis,
        output_basis,
        value_weight,
        output_weight.T,
        value_mean,
        value_square,
        output_mean,
        output_square,
    )
    out = pl.pallas_call(
        store,
        out_shape=shapes,
        in_specs=[vmem] * len(shapes),
        out_specs=(vmem,) * len(shapes),
        compiler_params=pltpu.CompilerParams(vmem_limit_bytes=16 * 1024 * 1024),
    )(*out)
    out = list(out)
    out[5], out[7] = out[5].T, out[7].T
    return tuple(out)


def solution(mesh):
    return jax.shard_map(
        on_device,
        mesh=mesh,
        in_specs=(
            P("fs", None),
            P("fs", "tp"),
            P("fs", "tp"),
            P("fs", None),
            P("fs", "tp"),
            P("tp", "fs"),
            P("fs", None),
            P("fs", None),
            P(None, "tp"),
            P(None, "tp"),
            P("tp", None),
            P("tp", None),
        ),
        out_specs=(
            P("fs", "tp"),
            P(None, "tp"),
            P("fs", "tp"),
            P(None, "tp"),
            P(None, "tp"),
            P("tp", "fs"),
            P("tp", None),
            P("tp", "fs"),
            P("tp", None),
            P("tp", None),
        ),
        check_vma=False,
    )
```

```python
import functools
import math

import jax
import jax.numpy as jnp
from jax import lax
from jax.experimental import pallas as pl
from jax.experimental.pallas import tpu as pltpu
from jax.sharding import PartitionSpec as P

NZ, NY, NX, NC = 16, 4, 4, 2
MESH = pl.DeviceIdType.MESH
W_BOUND = 0.1875
W_SLOPE = 250.0 / W_BOUND
CHUNKS = 4
NEAR = (4, 12, 3, 13, 2, 14, 1, 15)
IN_ORDER = (0, 1, 15, 2, 14, 3, 13, 4, 12, 5, 11, 6, 10, 7, 9, 8)
RELAYED = {4: (4, 3, 2, 1), 12: (-3, -2, -1)}
LAG_Y, LAG_X = 5, 9
FAR_FIRST = (8, 7, 9, 6, 10, 5, 11, 4, 12, 3, 13, 2, 14, 1, 15)


def coded(weight):
    size = jnp.exp2(jnp.abs(weight) * W_SLOPE - 125.0)
    return jnp.where(weight < 0, -size, size).astype(jnp.bfloat16)


def decoded(code):
    code = code.astype(jnp.float32)
    size = (jnp.log2(jnp.abs(code)) + 125.0) * (1.0 / W_SLOPE)
    return jnp.where(code < 0, -size, size)


def kernel(
    scaling,
    entries,
    x_hbm,
    v_hbm,
    m_hbm,
    oc_hbm,
    vb_hbm,
    ob_hbm,
    vw_hbm,
    ow_hbm,
    vmean_hbm,
    vsq_hbm,
    omean_hbm,
    osq_hbm,
    vnext_out,
    vcopy_out,
    vstep_out,
    vmean_out,
    vsq_out,
    onext_out,
    ocopy_out,
    ostep_out,
    omean_out,
    osq_out,
    xs,
    ocs,
    vs,
    ms,
    basis,
    owned,
    weights,
    grads,
    ysend,
    yrecv,
    zsend,
    zrecv,
    lows,
    sums,
    small,
    vstate,
    ostate,
    load_sem,
    chunk_sem,
    bz_s,
    bz_r,
    by_s,
    by_r,
    bx_s,
    bx_r,
    bd_s,
    bd_r,
    ry_s,
    ry_r,
    rz_s,
    rz_r,
    az_s,
    az_r,
    ay_s,
    ay_r,
    cl_s,
    cl_r,
    wz_s,
    wz_r,
    wy_s,
    wy_r,
):
    fs, tp = lax.axis_index("fs"), lax.axis_index("tp")
    z, y = fs // NY, lax.rem(fs, NY)
    x, c = tp // NC, lax.rem(tp, NC)
    parity = lax.rem(x, 2)
    tokens, width = xs.shape
    rank = basis.shape[3]
    local = vs.shape[1]
    rows = basis.shape[2]

    def zdev(zz):
        return {"fs": zz * NY + y, "tp": tp}

    def ydev(yy):
        return {"fs": z * NY + yy, "tp": tp}

    def xdev(xx):
        return {"fs": fs, "tp": xx * NC + c}

    sibling = {"fs": fs, "tp": x * NC + 1 - c}

    def zup(j):
        return lax.rem(z + j, NZ)

    def yup(j):
        return lax.rem(y + j, NY)

    def xup(j):
        return lax.rem(x + j, NX)

    pending = []

    def go(copy):
        copy.start()
        pending.append(copy)

    def remote(src, dst, ssem, rsem, device):
        return pltpu.make_async_remote_copy(
            src_ref=src, dst_ref=dst, send_sem=ssem, recv_sem=rsem, device_id=device, device_id_type=MESH
        )

    here = y * (NX * NC) + tp

    def plane(j):
        other = lax.rem(here + j, NY * NX * NC)
        return {"fs": z * NY + other // (NX * NC), "tp": lax.rem(other, NX * NC)}

    half = rows // 2

    def part_of(p):
        return pl.ds(pl.multiple_of(p * half, half), half)

    for k, far in enumerate((vb_hbm, ob_hbm)):

        @pl.when(c == k)
        def _(k=k, far=far):
            pltpu.make_async_copy(far.at[part_of(parity)], basis.at[k, fs, part_of(parity)], load_sem.at[0]).start()

    pltpu.make_async_copy(vw_hbm, owned.at[0], load_sem.at[1]).start()
    pltpu.make_async_copy(ow_hbm, owned.at[1], load_sem.at[8]).start()
    pltpu.make_async_copy(v_hbm, vs, load_sem.at[2]).start()
    pltpu.make_async_copy(m_hbm, ms, load_sem.at[3]).start()
    size = tokens // CHUNKS
    for t in range(CHUNKS):
        at = pl.ds(t * size, size)
        pltpu.make_async_copy(x_hbm.at[at], xs.at[at], chunk_sem.at[0, t]).start()
        pltpu.make_async_copy(oc_hbm.at[at], ocs.at[at], chunk_sem.at[1, t]).start()
    pltpu.make_async_copy(vmean_hbm, vstate.at[0], load_sem.at[4]).start()
    pltpu.make_async_copy(vsq_hbm, vstate.at[1], load_sem.at[5]).start()
    pltpu.make_async_copy(omean_hbm, ostate.at[0], load_sem.at[6]).start()
    pltpu.make_async_copy(osq_hbm, ostate.at[1], load_sem.at[7]).start()

    barrier = pltpu.get_barrier_semaphore()
    for j in NEAR:
        pl.semaphore_signal(barrier, inc=1, device_id=zdev(zup(j)), device_id_type=MESH)
    for j in range(1, NY * NX * NC):
        pl.semaphore_signal(barrier, inc=1, device_id=plane(j), device_id_type=MESH)

    pltpu.make_async_copy(vb_hbm.at[part_of(0)], basis.at[c, fs, part_of(parity)], load_sem.at[0]).wait()
    pltpu.make_async_copy(vw_hbm, owned.at[0], load_sem.at[1]).wait()
    pltpu.make_async_copy(ow_hbm, owned.at[1], load_sem.at[8]).wait()
    weights[fs] = coded(owned[...])

    pltpu.make_async_copy(v_hbm, vs, load_sem.at[2]).wait()
    pltpu.make_async_copy(m_hbm, ms, load_sem.at[3]).wait()
    across = (((0,), (0,)), ((), ()))
    for t in range(CHUNKS):
        at = pl.ds(t * size, size)
        for k, (far, near, thin) in enumerate(((x_hbm, xs, vs), (oc_hbm, ocs, ms))):
            pltpu.make_async_copy(far.at[at], near.at[at], chunk_sem.at[k, t]).wait()
            part = lax.dot_general(thin[at, :], near[at, :], across, preferred_element_type=jnp.float32)
            if t == 0:
                grads[k] = part
            else:
                grads[k] += part

    pl.semaphore_wait(barrier, len(NEAR) + NY * NX * NC - 1)

    def relay(block_of, ssem, rsem):
        def down(d, to):
            block = block_of(zup(NZ - d if d else 0))
            at = (d + to) % NZ - 1
            return remote(block, block, ssem.at[at], rsem.at[at], zdev(zup(to % NZ)))

        def arrived(d):
            block = block_of(zup(NZ - d))
            remote(block, block, ssem.at[d - 1], rsem.at[d - 1], zdev(zup(1))).wait_recv()

        return down, arrived

    def basis_row(zz):
        return basis.at[c, zz * NY + y, part_of(parity)]

    def weight_row(zz):
        return weights.at[zz * NY + y]

    send_basis, basis_came = relay(basis_row, bz_s, bz_r)
    send_weight, weight_came = relay(weight_row, wz_s, wz_r)

    def by(d, j):
        block = basis_row(zup(NZ - d if d else 0))
        return remote(block, block, by_s.at[d, j - 1], by_r.at[d, j - 1], ydev(yup(j)))

    def by_recv(d, j):
        block = basis.at[c, zup(NZ - d if d else 0) * NY + yup(NY - j), part_of(parity)]
        return remote(block, block, by_s.at[d, j - 1], by_r.at[d, j - 1], ydev(yup(1)))

    pair = NY // 2

    def bx(d, w):
        block = basis.at[c, pl.ds(zup(NZ - d if d else 0) * NY + w * pair, pair), part_of(parity)]
        return remote(block, block, bx_s.at[d, w], bx_r.at[d, w], xdev(xup(1 if w == 0 else NX - 1)))

    def bx_recv(d, w):
        block = basis.at[c, pl.ds(zup(NZ - d if d else 0) * NY + w * pair, pair), part_of(1 - parity)]
        return remote(block, block, bx_s.at[d, w], bx_r.at[d, w], xdev(xup(1)))

    def bd(d, w):
        block = basis.at[c, pl.ds(zup(NZ - d if d else 0) * NY, NY), part_of(parity if w == 0 else 1 - parity)]
        return remote(block, block, bd_s.at[d, w], bd_r.at[d, w], sibling)

    def bd_recv(d, w):
        block = basis.at[1 - c, pl.ds(zup(NZ - d if d else 0) * NY, NY), part_of(parity if w == 0 else 1 - parity)]
        return remote(block, block, bd_s.at[d, w], bd_r.at[d, w], sibling)

    for to in NEAR:
        go(send_basis(0, to))
    for s in range(NZ + LAG_X):
        if s < NZ:
            d = IN_ORDER[s]
            if d:
                basis_came(d)
            if d in RELAYED:
                for to in RELAYED[d]:
                    go(send_basis(d, to))
            for j in (2, 1, 3):
                go(by(d, j))
        if 0 <= s - LAG_Y < NZ:
            d = IN_ORDER[s - LAG_Y]
            for j in range(1, NY):
                by_recv(d, j).wait_recv()
            for w in range(2):
                go(bx(d, w))
            go(bd(d, 0))
        if s == NZ:
            for to in NEAR:
                go(send_weight(0, to))
        if 0 <= s - LAG_X < NZ:
            d = IN_ORDER[s - LAG_X]
            for w in range(2):
                bx_recv(d, w).wait_recv()
            go(bd(d, 1))

    def wy(d, j):
        block = weight_row(zup(NZ - d if d else 0))
        return remote(block, block, wy_s.at[d, j - 1], wy_r.at[d, j - 1], ydev(yup(j)))

    def wy_recv(d, j):
        block = weights.at[zup(NZ - d if d else 0) * NY + yup(NY - j)]
        return remote(block, block, wy_s.at[d, j - 1], wy_r.at[d, j - 1], ydev(yup(1)))

    for d in IN_ORDER:
        for w in range(2):
            bd_recv(d, w).wait_recv()

    quarter = local // NY
    for k in range(2):
        whole = grads[k]
        high = whole.astype(jnp.bfloat16)
        low = (whole - high.astype(jnp.float32)).astype(jnp.bfloat16)
        base = basis[k].reshape(-1, rank)
        part = jnp.dot(high, base, preferred_element_type=jnp.float32) + jnp.dot(
            low, base, preferred_element_type=jnp.float32
        )
        ysend[k] = (part * scaling).reshape(NY, quarter, rank)
        for j in (2, 1, 3):
            go(
                remote(
                    ysend.at[k, yup(j)], yrecv.at[k, j - 1], ry_s.at[k, j - 1], ry_r.at[k, j - 1], ydev(yup(j))
                )
            )

    for d in IN_ORDER[1:9]:
        weight_came(d)
        for to in RELAYED.get(d, ()):
            go(send_weight(d, to))

    def ry_recv(k, j):
        return remote(ysend.at[k, 0], yrecv.at[k, j - 1], ry_s.at[k, j - 1], ry_r.at[k, j - 1], ydev(yup(j)))

    piece = 2 * quarter // NZ
    for k in range(2):
        for j in range(1, NY):
            ry_recv(k, j).wait_recv()
        total = (ysend[k, y] + yrecv[k, 0]) + (yrecv[k, 1] + yrecv[k, 2])
        for i in range(NZ // 2):
            zsend[k * (NZ // 2) + i] = total[i * piece : (i + 1) * piece]

    def rz(j):
        return remote(zsend.at[zup(j)], zrecv.at[j - 1], rz_s.at[j - 1], rz_r.at[j - 1], zdev(zup(j)))

    for j in FAR_FIRST:
        go(rz(j))
    for d in IN_ORDER[:9]:
        for j in (2, 1, 3):
            go(wy(d, j))
    total = zsend[z]
    for j in reversed(FAR_FIRST):
        rz(j).wait_recv()
        total = total + zrecv[j - 1]
    lows[y, z] = total.astype(jnp.bfloat16)

    def az(j):
        block = lows.at[y, z]
        return remote(block, block, az_s.at[j - 1], az_r.at[j - 1], zdev(zup(j)))

    def az_recv(j):
        block = lows.at[y, zup(NZ - j)]
        return remote(block, block, az_s.at[j - 1], az_r.at[j - 1], zdev(zup(1)))

    for j in FAR_FIRST:
        go(az(j))
    for d in IN_ORDER[9:]:
        weight_came(d)
        for j in (2, 1, 3):
            go(wy(d, j))
    for j in reversed(FAR_FIRST):
        az_recv(j).wait_recv()

    def ay(j):
        block = lows.at[y]
        return remote(block, block, ay_s.at[j - 1], ay_r.at[j - 1], ydev(yup(j)))

    def ay_recv(j):
        block = lows.at[yup(NY - j)]
        return remote(block, block, ay_s.at[j - 1], ay_r.at[j - 1], ydev(yup(1)))

    for j in (2, 1, 3):
        go(ay(j))

    mine = lows[y].astype(jnp.float32)
    square = jnp.sum(mine * mine)
    sums[here] = jnp.full((1, 128), square, jnp.float32)

    def cl(j):
        block = sums.at[here]
        return remote(block, block, cl_s.at[j - 1], cl_r.at[j - 1], plane(j))

    def cl_recv(j):
        block = sums.at[lax.rem(here + NY * NX * NC - j, NY * NX * NC)]
        return remote(block, block, cl_s.at[j - 1], cl_r.at[j - 1], plane(1))

    for j in range(1, NY * NX * NC):
        go(cl(j))
    for j in (1, 3, 2):
        ay_recv(j).wait_recv()
    for k in range(2):
        for yy in range(NY):
            for i in range(NZ // 2):
                at = yy * quarter + i * piece
                small[k, at : at + piece, :] = lows[yy, k * (NZ // 2) + i].astype(jnp.float32)
    for j in range(1, NY * NX * NC):
        cl_recv(j).wait_recv()
    everyone = jnp.sum(sums[...], axis=0)
    clip = 1.0 / jnp.sqrt(1.0 + everyone[:, 0:1] / entries)

    for i, (far, near) in enumerate(
        (
            (vmean_hbm, vstate.at[0]),
            (vsq_hbm, vstate.at[1]),
            (omean_hbm, ostate.at[0]),
            (osq_hbm, ostate.at[1]),
        )
    ):
        pltpu.make_async_copy(far, near, load_sem.at[4 + i]).wait()

    def advance(low, state, mean_out, sq_out):
        scaled = low * clip
        mean = 0.8 * state[0] + 0.2 * scaled
        sq = 0.9 * state[1] + 0.1 * scaled * scaled
        mean_out[...] = mean
        sq_out[...] = sq
        return mean / jnp.sqrt(sq + 0.1)

    norms = (
        advance(small[0].T, vstate, vmean_out, vsq_out),
        advance(small[1], ostate, omean_out, osq_out).T,
    )
    for d in IN_ORDER:
        for j in range(1, NY):
            wy_recv(d, j).wait_recv()
    block_rows = 256
    per = block_rows // rows
    for k in range(2):
        high = norms[k].astype(jnp.bfloat16)
        low = (norms[k] - high.astype(jnp.float32)).astype(jnp.bfloat16)
        both = jnp.concatenate([high, low], axis=1)
        for b in range(width // block_rows):
            base = basis[k, b * per : (b + 1) * per].reshape(block_rows, rank)
            step = jnp.dot(base, both, preferred_element_type=jnp.float32)
            step = step[:, :local] + step[:, local:]
            weight = decoded(weights[b * per : (b + 1) * per, k].reshape(block_rows, local))
            moved = weight - 0.02 * step
            at = slice(b * block_rows, (b + 1) * block_rows)
            if k == 0:
                vcopy_out[at, :] = moved.astype(jnp.bfloat16)
            else:
                ocopy_out[:, at] = moved.T.astype(jnp.bfloat16)
        step = jnp.dot(basis[k, fs], both, preferred_element_type=jnp.float32)
        step = step[:, :local] + step[:, local:]
        (vstep_out, ostep_out)[k][...] = step
        (vnext_out, onext_out)[k][...] = owned[k] - 0.02 * step

    for copy in pending:
        copy.wait_send()


def store(*refs):
    count = len(refs) // 2
    for near, far in zip(refs[:count], refs[count:]):
        far[...] = near[...]


def on_device(
    block_input,
    value_cotangent,
    mixed_output,
    output_cotangent,
    value_weight,
    output_weight,
    value_basis,
    output_basis,
    value_mean,
    value_square,
    output_mean,
    output_square,
):
    tokens, width = block_input.shape
    local = value_cotangent.shape[1]
    rows, rank = value_basis.shape
    devices = lax.axis_size("fs")
    scaling = 1.0 / math.sqrt(tokens * devices)
    entries = 2.0 * rank * local * lax.axis_size("tp")
    quarter = local // NY
    piece = 2 * quarter // NZ
    f32, bf16 = jnp.float32, jnp.bfloat16
    hbm = pl.BlockSpec(memory_space=pltpu.HBM)
    vmem = pl.BlockSpec(memory_space=pltpu.VMEM)
    dma = pltpu.SemaphoreType.DMA
    near = NY * NX * NC - 1
    shapes = (
        jax.ShapeDtypeStruct((rows, local), f32),
        jax.ShapeDtypeStruct((width, local), bf16),
        jax.ShapeDtypeStruct((rows, local), f32),
        jax.ShapeDtypeStruct((rank, local), f32),
        jax.ShapeDtypeStruct((rank, local), f32),
        jax.ShapeDtypeStruct((rows, local), f32),
        jax.ShapeDtypeStruct((local, width), bf16),
        jax.ShapeDtypeStruct((rows, local), f32),
        jax.ShapeDtypeStruct((local, rank), f32),
        jax.ShapeDtypeStruct((local, rank), f32),
    )
    out = pl.pallas_call(
        functools.partial(kernel, scaling, entries),
        out_shape=shapes,
        in_specs=[hbm] * 12,
        out_specs=(vmem,) * len(shapes),
        scratch_shapes=[
            pltpu.VMEM((tokens, width), bf16),
            pltpu.VMEM((tokens, width), bf16),
            pltpu.VMEM((tokens, local), bf16),
            pltpu.VMEM((tokens, local), bf16),
            pltpu.VMEM((2, devices, rows, rank), bf16),
            pltpu.VMEM((2, rows, local), f32),
            pltpu.VMEM((devices, 2, rows, local), bf16),
            pltpu.VMEM((2, local, width), f32),
            pltpu.VMEM((2, NY, quarter, rank), f32),
            pltpu.VMEM((2, NY - 1, quarter, rank), f32),
            pltpu.VMEM((NZ, piece, rank), f32),
            pltpu.VMEM((NZ - 1, piece, rank), f32),
            pltpu.VMEM((NY, NZ, piece, rank), bf16),
            pltpu.VMEM((NY * NX * NC, 1, 128), f32),
            pltpu.VMEM((2, local, rank), f32),
            pltpu.VMEM((2, rank, local), f32),
            pltpu.VMEM((2, local, rank), f32),
            dma((9,)),
            dma((2, CHUNKS)),
            *[dma((NZ - 1,))] * 2,
            *[dma((NZ, NY - 1))] * 2,
            *[dma((NZ, 2))] * 4,
            *[dma((2, NY - 1))] * 2,
            *[dma((NZ - 1,))] * 4,
            *[dma((NY - 1,))] * 2,
            *[dma((near,))] * 2,
            *[dma((NZ - 1,))] * 2,
            *[dma((NZ, NY - 1))] * 2,
        ],
        compiler_params=pltpu.CompilerParams(
            collective_id=0, has_side_effects=True, vmem_limit_bytes=32 * 1024 * 1024
        ),
    )(
        *(
            pltpu.with_memory_space_constraint(a, pltpu.HBM)
            for a in (
                block_input,
                value_cotangent,
                mixed_output,
                output_cotangent,
                value_basis,
                output_basis,
                value_weight,
                output_weight.T,
                value_mean,
                value_square,
                output_mean,
                output_square,
            )
        )
    )
    out = pl.pallas_call(
        store,
        out_shape=shapes,
        in_specs=[vmem] * len(shapes),
        out_specs=(vmem,) * len(shapes),
        compiler_params=pltpu.CompilerParams(vmem_limit_bytes=16 * 1024 * 1024),
    )(*out)
    out = list(out)
    out[5], out[7] = out[5].T, out[7].T
    return tuple(out)


def solution(mesh):
    return jax.shard_map(
        on_device,
        mesh=mesh,
        in_specs=(
            P("fs", None),
            P("fs", "tp"),
            P("fs", "tp"),
            P("fs", None),
            P("fs", "tp"),
            P("tp", "fs"),
            P("fs", None),
            P("fs", None),
            P(None, "tp"),
            P(None, "tp"),
            P("tp", None),
            P("tp", None),
        ),
        out_specs=(
            P("fs", "tp"),
            P(None, "tp"),
            P("fs", "tp"),
            P(None, "tp"),
            P(None, "tp"),
            P("tp", "fs"),
            P("tp", None),
            P("tp", "fs"),
            P("tp", None),
            P("tp", None),
        ),
        check_vma=False,
    )
```

```python
import functools
import math

import jax
import jax.numpy as jnp
from jax import lax
from jax.experimental import pallas as pl
from jax.experimental.pallas import tpu as pltpu
from jax.sharding import PartitionSpec as P

NZ, NY, NX, NC = 16, 4, 4, 2
MESH = pl.DeviceIdType.MESH
W_BOUND = 0.1875
W_SLOPE = 250.0 / W_BOUND
CHUNKS = 4
NEAR = (4, 12, 3, 13, 2, 14, 1, 15)
IN_ORDER = (0, 1, 15, 2, 14, 3, 13, 4, 12, 5, 11, 6, 10, 7, 9, 8)
RELAYED = {4: (4, 3, 2, 1), 12: (-3, -2, -1)}
LAG_Y, LAG_X = 8, 14
PRODUCTS = 8
FAR_FIRST = (8, 7, 9, 6, 10, 5, 11, 4, 12, 3, 13, 2, 14, 1, 15)


def coded(weight):
    size = jnp.exp2(jnp.abs(weight) * W_SLOPE - 125.0)
    return jnp.where(weight < 0, -size, size).astype(jnp.bfloat16)


def decoded(code):
    code = code.astype(jnp.float32)
    size = (jnp.log2(jnp.abs(code)) + 125.0) * (1.0 / W_SLOPE)
    return jnp.where(code < 0, -size, size)


def kernel(
    scaling,
    entries,
    x_hbm,
    v_hbm,
    m_hbm,
    oc_hbm,
    vb_hbm,
    ob_hbm,
    vw_hbm,
    ow_hbm,
    vmean_hbm,
    vsq_hbm,
    omean_hbm,
    osq_hbm,
    vnext_out,
    vcopy_out,
    vstep_out,
    vmean_out,
    vsq_out,
    onext_out,
    ocopy_out,
    ostep_out,
    omean_out,
    osq_out,
    xs,
    ocs,
    vs,
    ms,
    basis,
    owned,
    weights,
    grads,
    ysend,
    yrecv,
    zsend,
    zrecv,
    lows,
    sums,
    quarters,
    small,
    vstate,
    ostate,
    load_sem,
    chunk_sem,
    bz_s,
    bz_r,
    by_s,
    by_r,
    bx_s,
    bx_r,
    bd_s,
    bd_r,
    ry_s,
    ry_r,
    rz_s,
    rz_r,
    az_s,
    az_r,
    ay_s,
    ay_r,
    cl_s,
    cl_r,
    cy_s,
    cy_r,
    wz_s,
    wz_r,
    wy_s,
    wy_r,
):
    fs, tp = lax.axis_index("fs"), lax.axis_index("tp")
    z, y = fs // NY, lax.rem(fs, NY)
    x, c = tp // NC, lax.rem(tp, NC)
    parity = lax.rem(x, 2)
    tokens, width = xs.shape
    rank = basis.shape[3]
    local = vs.shape[1]
    rows = basis.shape[2]

    def zdev(zz):
        return {"fs": zz * NY + y, "tp": tp}

    def ydev(yy):
        return {"fs": z * NY + yy, "tp": tp}

    def xdev(xx):
        return {"fs": fs, "tp": xx * NC + c}

    sibling = {"fs": fs, "tp": x * NC + 1 - c}

    def zup(j):
        return lax.rem(z + j, NZ)

    def yup(j):
        return lax.rem(y + j, NY)

    def xup(j):
        return lax.rem(x + j, NX)

    pending = []

    def go(copy):
        copy.start()
        pending.append(copy)

    def remote(src, dst, ssem, rsem, device):
        return pltpu.make_async_remote_copy(
            src_ref=src, dst_ref=dst, send_sem=ssem, recv_sem=rsem, device_id=device, device_id_type=MESH
        )

    def tdev(j):
        return {"fs": fs, "tp": lax.rem(tp + j, NX * NC)}

    half = rows // 2

    def part_of(p):
        return pl.ds(pl.multiple_of(p * half, half), half)

    for k, far in enumerate((vb_hbm, ob_hbm)):

        @pl.when(c == k)
        def _(k=k, far=far):
            pltpu.make_async_copy(far.at[part_of(parity)], basis.at[k, fs, part_of(parity)], load_sem.at[0]).start()

    pltpu.make_async_copy(vw_hbm, owned.at[0], load_sem.at[1]).start()
    pltpu.make_async_copy(ow_hbm, owned.at[1], load_sem.at[8]).start()
    pltpu.make_async_copy(v_hbm, vs, load_sem.at[2]).start()
    pltpu.make_async_copy(m_hbm, ms, load_sem.at[3]).start()
    size = tokens // CHUNKS
    for t in range(CHUNKS):
        at = pl.ds(t * size, size)
        pltpu.make_async_copy(x_hbm.at[at], xs.at[at], chunk_sem.at[0, t]).start()
        pltpu.make_async_copy(oc_hbm.at[at], ocs.at[at], chunk_sem.at[1, t]).start()
    pltpu.make_async_copy(vmean_hbm, vstate.at[0], load_sem.at[4]).start()
    pltpu.make_async_copy(vsq_hbm, vstate.at[1], load_sem.at[5]).start()
    pltpu.make_async_copy(omean_hbm, ostate.at[0], load_sem.at[6]).start()
    pltpu.make_async_copy(osq_hbm, ostate.at[1], load_sem.at[7]).start()

    barrier = pltpu.get_barrier_semaphore()
    for j in NEAR:
        pl.semaphore_signal(barrier, inc=1, device_id=zdev(zup(j)), device_id_type=MESH)
    for j in range(1, NY):
        pl.semaphore_signal(barrier, inc=1, device_id=ydev(yup(j)), device_id_type=MESH)
    for j in range(1, NX * NC):
        pl.semaphore_signal(barrier, inc=1, device_id=tdev(j), device_id_type=MESH)

    pltpu.make_async_copy(vb_hbm.at[part_of(0)], basis.at[c, fs, part_of(parity)], load_sem.at[0]).wait()
    pltpu.make_async_copy(vw_hbm, owned.at[0], load_sem.at[1]).wait()
    pltpu.make_async_copy(ow_hbm, owned.at[1], load_sem.at[8]).wait()
    weights[fs] = coded(owned[...])

    pl.semaphore_wait(barrier, len(NEAR) + NY - 1 + NX * NC - 1)

    across = (((0,), (0,)), ((), ()))

    def gradient(k, t):
        far, near, thin = ((x_hbm, xs, vs), (oc_hbm, ocs, ms))[k]
        at = pl.ds(t * size, size)
        if t == 0:
            pltpu.make_async_copy((v_hbm, m_hbm)[k], thin, load_sem.at[2 + k]).wait()
        pltpu.make_async_copy(far.at[at], near.at[at], chunk_sem.at[k, t]).wait()
        part = lax.dot_general(thin[at, :], near[at, :], across, preferred_element_type=jnp.float32)
        if t == 0:
            grads[k] = part
        else:
            grads[k] += part

    def relay(block_of, ssem, rsem):
        def down(d, to):
            block = block_of(zup(NZ - d if d else 0))
            at = (d + to) % NZ - 1
            return remote(block, block, ssem.at[at], rsem.at[at], zdev(zup(to % NZ)))

        def arrived(d):
            block = block_of(zup(NZ - d))
            remote(block, block, ssem.at[d - 1], rsem.at[d - 1], zdev(zup(1))).wait_recv()

        return down, arrived

    def basis_row(zz):
        return basis.at[c, zz * NY + y, part_of(parity)]

    def weight_row(zz):
        return weights.at[zz * NY + y]

    send_basis, basis_came = relay(basis_row, bz_s, bz_r)
    send_weight, weight_came = relay(weight_row, wz_s, wz_r)

    def by(d, j):
        block = basis_row(zup(NZ - d if d else 0))
        return remote(block, block, by_s.at[d, j - 1], by_r.at[d, j - 1], ydev(yup(j)))

    def by_recv(d, j):
        block = basis.at[c, zup(NZ - d if d else 0) * NY + yup(NY - j), part_of(parity)]
        return remote(block, block, by_s.at[d, j - 1], by_r.at[d, j - 1], ydev(yup(1)))

    pair = NY // 2

    def bx(d, w):
        block = basis.at[c, pl.ds(zup(NZ - d if d else 0) * NY + w * pair, pair), part_of(parity)]
        return remote(block, block, bx_s.at[d, w], bx_r.at[d, w], xdev(xup(1 if w == 0 else NX - 1)))

    def bx_recv(d, w):
        block = basis.at[c, pl.ds(zup(NZ - d if d else 0) * NY + w * pair, pair), part_of(1 - parity)]
        return remote(block, block, bx_s.at[d, w], bx_r.at[d, w], xdev(xup(1)))

    def bd(d, w):
        block = basis.at[c, pl.ds(zup(NZ - d if d else 0) * NY, NY), part_of(parity if w == 0 else 1 - parity)]
        return remote(block, block, bd_s.at[d, w], bd_r.at[d, w], sibling)

    def bd_recv(d, w):
        block = basis.at[1 - c, pl.ds(zup(NZ - d if d else 0) * NY, NY), part_of(parity if w == 0 else 1 - parity)]
        return remote(block, block, bd_s.at[d, w], bd_r.at[d, w], sibling)

    for to in NEAR:
        go(send_basis(0, to))
    for s in range(NZ + LAG_X):
        if s < NZ:
            d = IN_ORDER[s]
            if d:
                basis_came(d)
            if d in RELAYED:
                for to in RELAYED[d]:
                    go(send_basis(d, to))
            for j in (2, 1, 3):
                go(by(d, j))
        if 0 <= s - PRODUCTS < 2 * CHUNKS:
            gradient((s - PRODUCTS) % 2, (s - PRODUCTS) // 2)
        if 0 <= s - LAG_Y < NZ:
            d = IN_ORDER[s - LAG_Y]
            for j in range(1, NY):
                by_recv(d, j).wait_recv()
            for w in range(2):
                go(bx(d, w))
            go(bd(d, 0))
        if s == NZ:
            for to in NEAR:
                go(send_weight(0, to))
        if 0 <= s - LAG_X < NZ:
            d = IN_ORDER[s - LAG_X]
            for w in range(2):
                bx_recv(d, w).wait_recv()
            go(bd(d, 1))

    def wy(d, j):
        block = weight_row(zup(NZ - d if d else 0))
        return remote(block, block, wy_s.at[d, j - 1], wy_r.at[d, j - 1], ydev(yup(j)))

    def wy_recv(d, j):
        block = weights.at[zup(NZ - d if d else 0) * NY + yup(NY - j)]
        return remote(block, block, wy_s.at[d, j - 1], wy_r.at[d, j - 1], ydev(yup(1)))

    for d in IN_ORDER:
        for w in range(2):
            bd_recv(d, w).wait_recv()

    quarter = local // NY
    for k in range(2):
        whole = grads[k]
        high = whole.astype(jnp.bfloat16)
        low = (whole - high.astype(jnp.float32)).astype(jnp.bfloat16)
        base = basis[k].reshape(-1, rank)
        part = jnp.dot(high, base, preferred_element_type=jnp.float32) + jnp.dot(
            low, base, preferred_element_type=jnp.float32
        )
        ysend[k] = (part * scaling).reshape(NY, quarter, rank)
        for j in (2, 1, 3):
            go(
                remote(
                    ysend.at[k, yup(j)], yrecv.at[k, j - 1], ry_s.at[k, j - 1], ry_r.at[k, j - 1], ydev(yup(j))
                )
            )

    for d in IN_ORDER[1:9]:
        weight_came(d)
        for to in RELAYED.get(d, ()):
            go(send_weight(d, to))

    def ry_recv(k, j):
        return remote(ysend.at[k, 0], yrecv.at[k, j - 1], ry_s.at[k, j - 1], ry_r.at[k, j - 1], ydev(yup(j)))

    piece = 2 * quarter // NZ
    for k in range(2):
        for j in range(1, NY):
            ry_recv(k, j).wait_recv()
        total = (ysend[k, y] + yrecv[k, 0]) + (yrecv[k, 1] + yrecv[k, 2])
        for i in range(NZ // 2):
            zsend[k * (NZ // 2) + i] = total[i * piece : (i + 1) * piece]

    def rz(j):
        return remote(zsend.at[zup(j)], zrecv.at[j - 1], rz_s.at[j - 1], rz_r.at[j - 1], zdev(zup(j)))

    for j in FAR_FIRST:
        go(rz(j))
    for d in IN_ORDER[:9]:
        for j in (2, 1, 3):
            go(wy(d, j))
    total = zsend[z]
    for j in reversed(FAR_FIRST):
        rz(j).wait_recv()
        total = total + zrecv[j - 1]
    lows[y, z] = total.astype(jnp.bfloat16)

    def az(j):
        block = lows.at[y, z]
        return remote(block, block, az_s.at[j - 1], az_r.at[j - 1], zdev(zup(j)))

    def az_recv(j):
        block = lows.at[y, zup(NZ - j)]
        return remote(block, block, az_s.at[j - 1], az_r.at[j - 1], zdev(zup(1)))

    for j in FAR_FIRST:
        go(az(j))
    for d in IN_ORDER[9:]:
        weight_came(d)
        for j in (2, 1, 3):
            go(wy(d, j))
    for j in reversed(FAR_FIRST):
        az_recv(j).wait_recv()

    def ay(j):
        block = lows.at[y]
        return remote(block, block, ay_s.at[j - 1], ay_r.at[j - 1], ydev(yup(j)))

    def ay_recv(j):
        block = lows.at[yup(NY - j)]
        return remote(block, block, ay_s.at[j - 1], ay_r.at[j - 1], ydev(yup(1)))

    for j in (2, 1, 3):
        go(ay(j))

    mine = lows[y].astype(jnp.float32)
    square = jnp.sum(mine * mine)
    sums[tp] = jnp.full((1, 128), square, jnp.float32)

    def cl(j):
        block = sums.at[tp]
        return remote(block, block, cl_s.at[j - 1], cl_r.at[j - 1], tdev(j))

    def cl_recv(j):
        block = sums.at[lax.rem(tp + NX * NC - j, NX * NC)]
        return remote(block, block, cl_s.at[j - 1], cl_r.at[j - 1], tdev(1))

    def cy(j):
        block = quarters.at[y]
        return remote(block, block, cy_s.at[j - 1], cy_r.at[j - 1], ydev(yup(j)))

    def cy_recv(j):
        block = quarters.at[yup(NY - j)]
        return remote(block, block, cy_s.at[j - 1], cy_r.at[j - 1], ydev(yup(1)))

    for j in range(1, NX * NC):
        go(cl(j))
    for j in range(1, NX * NC):
        cl_recv(j).wait_recv()
    quarters[y] = jnp.sum(sums[...], axis=0)
    for j in (2, 1, 3):
        go(cy(j))
    for j in (1, 3, 2):
        ay_recv(j).wait_recv()
    for k in range(2):
        for yy in range(NY):
            for i in range(NZ // 2):
                at = yy * quarter + i * piece
                small[k, at : at + piece, :] = lows[yy, k * (NZ // 2) + i].astype(jnp.float32)
    for j in range(1, NY):
        cy_recv(j).wait_recv()
    everyone = jnp.sum(quarters[...], axis=0)
    clip = 1.0 / jnp.sqrt(1.0 + everyone[:, 0:1] / entries)

    for i, (far, near) in enumerate(
        (
            (vmean_hbm, vstate.at[0]),
            (vsq_hbm, vstate.at[1]),
            (omean_hbm, ostate.at[0]),
            (osq_hbm, ostate.at[1]),
        )
    ):
        pltpu.make_async_copy(far, near, load_sem.at[4 + i]).wait()

    def advance(low, state, mean_out, sq_out):
        scaled = low * clip
        mean = 0.8 * state[0] + 0.2 * scaled
        sq = 0.9 * state[1] + 0.1 * scaled * scaled
        mean_out[...] = mean
        sq_out[...] = sq
        return mean / jnp.sqrt(sq + 0.1)

    norms = (
        advance(small[0].T, vstate, vmean_out, vsq_out),
        advance(small[1], ostate, omean_out, osq_out).T,
    )
    for d in IN_ORDER:
        for j in range(1, NY):
            wy_recv(d, j).wait_recv()
    block_rows = 256
    per = block_rows // rows
    for k in range(2):
        high = norms[k].astype(jnp.bfloat16)
        low = (norms[k] - high.astype(jnp.float32)).astype(jnp.bfloat16)
        both = jnp.concatenate([high, low], axis=1)
        for b in range(width // block_rows):
            base = basis[k, b * per : (b + 1) * per].reshape(block_rows, rank)
            step = jnp.dot(base, both, preferred_element_type=jnp.float32)
            step = step[:, :local] + step[:, local:]
            weight = decoded(weights[b * per : (b + 1) * per, k].reshape(block_rows, local))
            moved = weight - 0.02 * step
            at = slice(b * block_rows, (b + 1) * block_rows)
            if k == 0:
                vcopy_out[at, :] = moved.astype(jnp.bfloat16)
            else:
                ocopy_out[:, at] = moved.T.astype(jnp.bfloat16)
        step = jnp.dot(basis[k, fs], both, preferred_element_type=jnp.float32)
        step = step[:, :local] + step[:, local:]
        (vstep_out, ostep_out)[k][...] = step
        (vnext_out, onext_out)[k][...] = owned[k] - 0.02 * step

    for copy in pending:
        copy.wait_send()


def store(*refs):
    count = len(refs) // 2
    for near, far in zip(refs[:count], refs[count:]):
        far[...] = near[...]


def on_device(
    block_input,
    value_cotangent,
    mixed_output,
    output_cotangent,
    value_weight,
    output_weight,
    value_basis,
    output_basis,
    value_mean,
    value_square,
    output_mean,
    output_square,
):
    tokens, width = block_input.shape
    local = value_cotangent.shape[1]
    rows, rank = value_basis.shape
    devices = lax.axis_size("fs")
    scaling = 1.0 / math.sqrt(tokens * devices)
    entries = 2.0 * rank * local * lax.axis_size("tp")
    quarter = local // NY
    piece = 2 * quarter // NZ
    f32, bf16 = jnp.float32, jnp.bfloat16
    hbm = pl.BlockSpec(memory_space=pltpu.HBM)
    vmem = pl.BlockSpec(memory_space=pltpu.VMEM)
    dma = pltpu.SemaphoreType.DMA
    shapes = (
        jax.ShapeDtypeStruct((rows, local), f32),
        jax.ShapeDtypeStruct((width, local), bf16),
        jax.ShapeDtypeStruct((rows, local), f32),
        jax.ShapeDtypeStruct((rank, local), f32),
        jax.ShapeDtypeStruct((rank, local), f32),
        jax.ShapeDtypeStruct((rows, local), f32),
        jax.ShapeDtypeStruct((local, width), bf16),
        jax.ShapeDtypeStruct((rows, local), f32),
        jax.ShapeDtypeStruct((local, rank), f32),
        jax.ShapeDtypeStruct((local, rank), f32),
    )
    out = pl.pallas_call(
        functools.partial(kernel, scaling, entries),
        out_shape=shapes,
        in_specs=[hbm] * 12,
        out_specs=(vmem,) * len(shapes),
        scratch_shapes=[
            pltpu.VMEM((tokens, width), bf16),
            pltpu.VMEM((tokens, width), bf16),
            pltpu.VMEM((tokens, local), bf16),
            pltpu.VMEM((tokens, local), bf16),
            pltpu.VMEM((2, devices, rows, rank), bf16),
            pltpu.VMEM((2, rows, local), f32),
            pltpu.VMEM((devices, 2, rows, local), bf16),
            pltpu.VMEM((2, local, width), f32),
            pltpu.VMEM((2, NY, quarter, rank), f32),
            pltpu.VMEM((2, NY - 1, quarter, rank), f32),
            pltpu.VMEM((NZ, piece, rank), f32),
            pltpu.VMEM((NZ - 1, piece, rank), f32),
            pltpu.VMEM((NY, NZ, piece, rank), bf16),
            pltpu.VMEM((NX * NC, 1, 128), f32),
            pltpu.VMEM((NY, 1, 128), f32),
            pltpu.VMEM((2, local, rank), f32),
            pltpu.VMEM((2, rank, local), f32),
            pltpu.VMEM((2, local, rank), f32),
            dma((9,)),
            dma((2, CHUNKS)),
            *[dma((NZ - 1,))] * 2,
            *[dma((NZ, NY - 1))] * 2,
            *[dma((NZ, 2))] * 4,
            *[dma((2, NY - 1))] * 2,
            *[dma((NZ - 1,))] * 4,
            *[dma((NY - 1,))] * 2,
            *[dma((NX * NC - 1,))] * 2,
            *[dma((NY - 1,))] * 2,
            *[dma((NZ - 1,))] * 2,
            *[dma((NZ, NY - 1))] * 2,
        ],
        compiler_params=pltpu.CompilerParams(
            collective_id=0, has_side_effects=True, vmem_limit_bytes=32 * 1024 * 1024
        ),
    )(
        *(
            pltpu.with_memory_space_constraint(a, pltpu.HBM)
            for a in (
                block_input,
                value_cotangent,
                mixed_output,
                output_cotangent,
                value_basis,
                output_basis,
                value_weight,
                output_weight.T,
                value_mean,
                value_square,
                output_mean,
                output_square,
            )
        )
    )
    out = pl.pallas_call(
        store,
        out_shape=shapes,
        in_specs=[vmem] * len(shapes),
        out_specs=(vmem,) * len(shapes),
        compiler_params=pltpu.CompilerParams(vmem_limit_bytes=16 * 1024 * 1024),
    )(*out)
    out = list(out)
    out[5], out[7] = out[5].T, out[7].T
    return tuple(out)


def solution(mesh):
    return jax.shard_map(
        on_device,
        mesh=mesh,
        in_specs=(
            P("fs", None),
            P("fs", "tp"),
            P("fs", "tp"),
            P("fs", None),
            P("fs", "tp"),
            P("tp", "fs"),
            P("fs", None),
            P("fs", None),
            P(None, "tp"),
            P(None, "tp"),
            P("tp", None),
            P("tp", None),
        ),
        out_specs=(
            P("fs", "tp"),
            P(None, "tp"),
            P("fs", "tp"),
            P(None, "tp"),
            P(None, "tp"),
            P("tp", "fs"),
            P("tp", None),
            P("tp", "fs"),
            P("tp", None),
            P("tp", None),
        ),
        check_vma=False,
    )
```

```python
import functools
import math

import jax
import jax.numpy as jnp
from jax import lax
from jax.experimental import pallas as pl
from jax.experimental.pallas import tpu as pltpu
from jax.sharding import PartitionSpec as P

NZ, NY, NX, NC = 16, 4, 4, 2
MESH = pl.DeviceIdType.MESH
W_BOUND = 0.1875
W_SLOPE = 250.0 / W_BOUND
CHUNKS = 4
NEAR = (4, 12, 3, 13, 2, 14, 1, 15)
IN_ORDER = (0, 1, 15, 2, 14, 3, 13, 4, 12, 5, 11, 6, 10, 7, 9, 8)
RELAYED = {4: (4, 3, 2, 1), 12: (-3, -2, -1)}
LAG_Y, LAG_X = 8, 16
PRODUCTS = 8
FAR_FIRST = (8, 7, 9, 6, 10, 5, 11, 4, 12, 3, 13, 2, 14, 1, 15)


def coded(weight):
    size = jnp.exp2(jnp.abs(weight) * W_SLOPE - 125.0)
    return jnp.where(weight < 0, -size, size).astype(jnp.bfloat16)


def decoded(code):
    code = code.astype(jnp.float32)
    size = (jnp.log2(jnp.abs(code)) + 125.0) * (1.0 / W_SLOPE)
    return jnp.where(code < 0, -size, size)


def kernel(
    scaling,
    entries,
    x_hbm,
    v_hbm,
    m_hbm,
    oc_hbm,
    vb_hbm,
    ob_hbm,
    vw_hbm,
    ow_hbm,
    vmean_hbm,
    vsq_hbm,
    omean_hbm,
    osq_hbm,
    vnext_out,
    vcopy_out,
    vstep_out,
    vmean_out,
    vsq_out,
    onext_out,
    ocopy_out,
    ostep_out,
    omean_out,
    osq_out,
    xs,
    ocs,
    vs,
    ms,
    basis,
    owned,
    weights,
    grads,
    ysend,
    yrecv,
    zsend,
    zrecv,
    lows,
    sums,
    quarters,
    small,
    vstate,
    ostate,
    load_sem,
    chunk_sem,
    bz_s,
    bz_r,
    by_s,
    by_r,
    bx_s,
    bx_r,
    bd_s,
    bd_r,
    ry_s,
    ry_r,
    rz_s,
    rz_r,
    az_s,
    az_r,
    ay_s,
    ay_r,
    cl_s,
    cl_r,
    cy_s,
    cy_r,
    wz_s,
    wz_r,
    wy_s,
    wy_r,
):
    fs, tp = lax.axis_index("fs"), lax.axis_index("tp")
    z, y = fs // NY, lax.rem(fs, NY)
    x, c = tp // NC, lax.rem(tp, NC)
    parity = lax.rem(x, 2)
    tokens, width = xs.shape
    rank = basis.shape[3]
    local = vs.shape[1]
    rows = basis.shape[2]

    def zdev(zz):
        return {"fs": zz * NY + y, "tp": tp}

    def ydev(yy):
        return {"fs": z * NY + yy, "tp": tp}

    def xdev(xx):
        return {"fs": fs, "tp": xx * NC + c}

    sibling = {"fs": fs, "tp": x * NC + 1 - c}

    def zup(j):
        return lax.rem(z + j, NZ)

    def yup(j):
        return lax.rem(y + j, NY)

    def xup(j):
        return lax.rem(x + j, NX)

    pending = []

    def go(copy):
        copy.start()
        pending.append(copy)

    def remote(src, dst, ssem, rsem, device):
        return pltpu.make_async_remote_copy(
            src_ref=src, dst_ref=dst, send_sem=ssem, recv_sem=rsem, device_id=device, device_id_type=MESH
        )

    def tdev(j):
        return {"fs": fs, "tp": lax.rem(tp + j, NX * NC)}

    half = rows // 2

    def part_of(p):
        return pl.ds(pl.multiple_of(p * half, half), half)

    for k, far in enumerate((vb_hbm, ob_hbm)):

        @pl.when(c == k)
        def _(k=k, far=far):
            pltpu.make_async_copy(far.at[part_of(parity)], basis.at[k, fs, part_of(parity)], load_sem.at[0]).start()

    pltpu.make_async_copy(vw_hbm, owned.at[0], load_sem.at[1]).start()
    pltpu.make_async_copy(ow_hbm, owned.at[1], load_sem.at[8]).start()
    pltpu.make_async_copy(v_hbm, vs, load_sem.at[2]).start()
    pltpu.make_async_copy(m_hbm, ms, load_sem.at[3]).start()
    size = tokens // CHUNKS
    for t in range(CHUNKS):
        at = pl.ds(t * size, size)
        pltpu.make_async_copy(x_hbm.at[at], xs.at[at], chunk_sem.at[0, t]).start()
        pltpu.make_async_copy(oc_hbm.at[at], ocs.at[at], chunk_sem.at[1, t]).start()
    pltpu.make_async_copy(vmean_hbm, vstate.at[0], load_sem.at[4]).start()
    pltpu.make_async_copy(vsq_hbm, vstate.at[1], load_sem.at[5]).start()
    pltpu.make_async_copy(omean_hbm, ostate.at[0], load_sem.at[6]).start()
    pltpu.make_async_copy(osq_hbm, ostate.at[1], load_sem.at[7]).start()

    barrier = pltpu.get_barrier_semaphore()
    for j in NEAR:
        pl.semaphore_signal(barrier, inc=1, device_id=zdev(zup(j)), device_id_type=MESH)
    for j in range(1, NY):
        pl.semaphore_signal(barrier, inc=1, device_id=ydev(yup(j)), device_id_type=MESH)
    for j in range(1, NX * NC):
        pl.semaphore_signal(barrier, inc=1, device_id=tdev(j), device_id_type=MESH)

    pltpu.make_async_copy(vb_hbm.at[part_of(0)], basis.at[c, fs, part_of(parity)], load_sem.at[0]).wait()
    pltpu.make_async_copy(vw_hbm, owned.at[0], load_sem.at[1]).wait()
    pltpu.make_async_copy(ow_hbm, owned.at[1], load_sem.at[8]).wait()
    weights[fs] = coded(owned[...])

    pl.semaphore_wait(barrier, len(NEAR) + NY - 1 + NX * NC - 1)

    across = (((0,), (0,)), ((), ()))

    def gradient(k, t):
        far, near, thin = ((x_hbm, xs, vs), (oc_hbm, ocs, ms))[k]
        at = pl.ds(t * size, size)
        if t == 0:
            pltpu.make_async_copy((v_hbm, m_hbm)[k], thin, load_sem.at[2 + k]).wait()
        pltpu.make_async_copy(far.at[at], near.at[at], chunk_sem.at[k, t]).wait()
        part = lax.dot_general(thin[at, :], near[at, :], across, preferred_element_type=jnp.float32)
        if t == 0:
            grads[k] = part
        else:
            grads[k] += part

    def relay(block_of, ssem, rsem):
        def down(d, to):
            block = block_of(zup(NZ - d if d else 0))
            at = (d + to) % NZ - 1
            return remote(block, block, ssem.at[at], rsem.at[at], zdev(zup(to % NZ)))

        def arrived(d):
            block = block_of(zup(NZ - d))
            remote(block, block, ssem.at[d - 1], rsem.at[d - 1], zdev(zup(1))).wait_recv()

        return down, arrived

    def basis_row(zz):
        return basis.at[c, zz * NY + y, part_of(parity)]

    def weight_row(zz):
        return weights.at[zz * NY + y]

    send_basis, basis_came = relay(basis_row, bz_s, bz_r)
    send_weight, weight_came = relay(weight_row, wz_s, wz_r)

    def by(d, j):
        block = basis_row(zup(NZ - d if d else 0))
        return remote(block, block, by_s.at[d, j - 1], by_r.at[d, j - 1], ydev(yup(j)))

    def by_recv(d, j):
        block = basis.at[c, zup(NZ - d if d else 0) * NY + yup(NY - j), part_of(parity)]
        return remote(block, block, by_s.at[d, j - 1], by_r.at[d, j - 1], ydev(yup(1)))

    pair = NY // 2

    def bx(d, w):
        block = basis.at[c, pl.ds(zup(NZ - d if d else 0) * NY + w * pair, pair), part_of(parity)]
        return remote(block, block, bx_s.at[d, w], bx_r.at[d, w], xdev(xup(1 if w == 0 else NX - 1)))

    def bx_recv(d, w):
        block = basis.at[c, pl.ds(zup(NZ - d if d else 0) * NY + w * pair, pair), part_of(1 - parity)]
        return remote(block, block, bx_s.at[d, w], bx_r.at[d, w], xdev(xup(1)))

    def bd(d):
        block = basis.at[c, pl.ds(zup(NZ - d if d else 0) * NY, NY)]
        return remote(block, block, bd_s.at[d], bd_r.at[d], sibling)

    def bd_recv(d):
        block = basis.at[1 - c, pl.ds(zup(NZ - d if d else 0) * NY, NY)]
        return remote(block, block, bd_s.at[d], bd_r.at[d], sibling)

    for to in NEAR:
        go(send_basis(0, to))
    for s in range(NZ + LAG_X):
        if s < NZ:
            d = IN_ORDER[s]
            if d:
                basis_came(d)
            if d in RELAYED:
                for to in RELAYED[d]:
                    go(send_basis(d, to))
            for j in (2, 1, 3):
                go(by(d, j))
        if 0 <= s - PRODUCTS < 2 * CHUNKS:
            gradient((s - PRODUCTS) % 2, (s - PRODUCTS) // 2)
        if 0 <= s - LAG_Y < NZ:
            d = IN_ORDER[s - LAG_Y]
            for j in range(1, NY):
                by_recv(d, j).wait_recv()
            for w in range(2):
                go(bx(d, w))
        if s == NZ:
            for to in NEAR:
                go(send_weight(0, to))
        if 0 <= s - LAG_X < NZ:
            d = IN_ORDER[s - LAG_X]
            for w in range(2):
                bx_recv(d, w).wait_recv()
            go(bd(d))

    def wy(d, j):
        block = weight_row(zup(NZ - d if d else 0))
        return remote(block, block, wy_s.at[d, j - 1], wy_r.at[d, j - 1], ydev(yup(j)))

    def wy_recv(d, j):
        block = weights.at[zup(NZ - d if d else 0) * NY + yup(NY - j)]
        return remote(block, block, wy_s.at[d, j - 1], wy_r.at[d, j - 1], ydev(yup(1)))

    quarter = local // NY
    for turn, k in enumerate((c, 1 - c)):
        if turn == 1:
            for d in IN_ORDER:
                bd_recv(d).wait_recv()
        whole = grads[k]
        high = whole.astype(jnp.bfloat16)
        low = (whole - high.astype(jnp.float32)).astype(jnp.bfloat16)
        base = basis[k].reshape(-1, rank)
        part = jnp.dot(high, base, preferred_element_type=jnp.float32) + jnp.dot(
            low, base, preferred_element_type=jnp.float32
        )
        ysend[k] = (part * scaling).reshape(NY, quarter, rank)
        for j in (2, 1, 3):
            go(
                remote(
                    ysend.at[k, yup(j)], yrecv.at[k, j - 1], ry_s.at[k, j - 1], ry_r.at[k, j - 1], ydev(yup(j))
                )
            )

    for d in IN_ORDER[1:9]:
        weight_came(d)
        for to in RELAYED.get(d, ()):
            go(send_weight(d, to))

    def ry_recv(k, j):
        return remote(ysend.at[k, 0], yrecv.at[k, j - 1], ry_s.at[k, j - 1], ry_r.at[k, j - 1], ydev(yup(j)))

    piece = 2 * quarter // NZ
    for k in range(2):
        for j in range(1, NY):
            ry_recv(k, j).wait_recv()
        total = (ysend[k, y] + yrecv[k, 0]) + (yrecv[k, 1] + yrecv[k, 2])
        for i in range(NZ // 2):
            zsend[k * (NZ // 2) + i] = total[i * piece : (i + 1) * piece]

    def rz(j):
        return remote(zsend.at[zup(j)], zrecv.at[j - 1], rz_s.at[j - 1], rz_r.at[j - 1], zdev(zup(j)))

    for j in FAR_FIRST:
        go(rz(j))
    for d in IN_ORDER[:9]:
        for j in (2, 1, 3):
            go(wy(d, j))
    total = zsend[z]
    for j in reversed(FAR_FIRST):
        rz(j).wait_recv()
        total = total + zrecv[j - 1]
    lows[y, z] = total.astype(jnp.bfloat16)

    def az(j):
        block = lows.at[y, z]
        return remote(block, block, az_s.at[j - 1], az_r.at[j - 1], zdev(zup(j)))

    def az_recv(j):
        block = lows.at[y, zup(NZ - j)]
        return remote(block, block, az_s.at[j - 1], az_r.at[j - 1], zdev(zup(1)))

    for j in FAR_FIRST:
        go(az(j))
    for d in IN_ORDER[9:]:
        weight_came(d)
        for j in (2, 1, 3):
            go(wy(d, j))
    for j in reversed(FAR_FIRST):
        az_recv(j).wait_recv()

    def ay(j):
        block = lows.at[y]
        return remote(block, block, ay_s.at[j - 1], ay_r.at[j - 1], ydev(yup(j)))

    def ay_recv(j):
        block = lows.at[yup(NY - j)]
        return remote(block, block, ay_s.at[j - 1], ay_r.at[j - 1], ydev(yup(1)))

    for j in (2, 1, 3):
        go(ay(j))

    mine = lows[y].astype(jnp.float32)
    square = jnp.sum(mine * mine)
    sums[tp] = jnp.full((1, 128), square, jnp.float32)

    def cl(j):
        block = sums.at[tp]
        return remote(block, block, cl_s.at[j - 1], cl_r.at[j - 1], tdev(j))

    def cl_recv(j):
        block = sums.at[lax.rem(tp + NX * NC - j, NX * NC)]
        return remote(block, block, cl_s.at[j - 1], cl_r.at[j - 1], tdev(1))

    def cy(j):
        block = quarters.at[y]
        return remote(block, block, cy_s.at[j - 1], cy_r.at[j - 1], ydev(yup(j)))

    def cy_recv(j):
        block = quarters.at[yup(NY - j)]
        return remote(block, block, cy_s.at[j - 1], cy_r.at[j - 1], ydev(yup(1)))

    for j in range(1, NX * NC):
        go(cl(j))
    for j in range(1, NX * NC):
        cl_recv(j).wait_recv()
    quarters[y] = jnp.sum(sums[...], axis=0)
    for j in (2, 1, 3):
        go(cy(j))
    for j in (1, 3, 2):
        ay_recv(j).wait_recv()
    for k in range(2):
        for yy in range(NY):
            for i in range(NZ // 2):
                at = yy * quarter + i * piece
                small[k, at : at + piece, :] = lows[yy, k * (NZ // 2) + i].astype(jnp.float32)
    for j in range(1, NY):
        cy_recv(j).wait_recv()
    everyone = jnp.sum(quarters[...], axis=0)
    clip = 1.0 / jnp.sqrt(1.0 + everyone[:, 0:1] / entries)

    for i, (far, near) in enumerate(
        (
            (vmean_hbm, vstate.at[0]),
            (vsq_hbm, vstate.at[1]),
            (omean_hbm, ostate.at[0]),
            (osq_hbm, ostate.at[1]),
        )
    ):
        pltpu.make_async_copy(far, near, load_sem.at[4 + i]).wait()

    def advance(low, state, mean_out, sq_out):
        scaled = low * clip
        mean = 0.8 * state[0] + 0.2 * scaled
        sq = 0.9 * state[1] + 0.1 * scaled * scaled
        mean_out[...] = mean
        sq_out[...] = sq
        return mean / jnp.sqrt(sq + 0.1)

    norms = (
        advance(small[0].T, vstate, vmean_out, vsq_out),
        advance(small[1], ostate, omean_out, osq_out).T,
    )
    for d in IN_ORDER:
        for j in range(1, NY):
            wy_recv(d, j).wait_recv()
    block_rows = 256
    per = block_rows // rows
    for k in range(2):
        high = norms[k].astype(jnp.bfloat16)
        low = (norms[k] - high.astype(jnp.float32)).astype(jnp.bfloat16)
        both = jnp.concatenate([high, low], axis=1)
        for b in range(width // block_rows):
            base = basis[k, b * per : (b + 1) * per].reshape(block_rows, rank)
            step = jnp.dot(base, both, preferred_element_type=jnp.float32)
            step = step[:, :local] + step[:, local:]
            weight = decoded(weights[b * per : (b + 1) * per, k].reshape(block_rows, local))
            moved = weight - 0.02 * step
            at = slice(b * block_rows, (b + 1) * block_rows)
            if k == 0:
                vcopy_out[at, :] = moved.astype(jnp.bfloat16)
            else:
                ocopy_out[:, at] = moved.T.astype(jnp.bfloat16)
        step = jnp.dot(basis[k, fs], both, preferred_element_type=jnp.float32)
        step = step[:, :local] + step[:, local:]
        (vstep_out, ostep_out)[k][...] = step
        (vnext_out, onext_out)[k][...] = owned[k] - 0.02 * step

    for copy in pending:
        copy.wait_send()


def store(*refs):
    count = len(refs) // 2
    for near, far in zip(refs[:count], refs[count:]):
        far[...] = near[...]


def on_device(
    block_input,
    value_cotangent,
    mixed_output,
    output_cotangent,
    value_weight,
    output_weight,
    value_basis,
    output_basis,
    value_mean,
    value_square,
    output_mean,
    output_square,
):
    tokens, width = block_input.shape
    local = value_cotangent.shape[1]
    rows, rank = value_basis.shape
    devices = lax.axis_size("fs")
    scaling = 1.0 / math.sqrt(tokens * devices)
    entries = 2.0 * rank * local * lax.axis_size("tp")
    quarter = local // NY
    piece = 2 * quarter // NZ
    f32, bf16 = jnp.float32, jnp.bfloat16
    hbm = pl.BlockSpec(memory_space=pltpu.HBM)
    vmem = pl.BlockSpec(memory_space=pltpu.VMEM)
    dma = pltpu.SemaphoreType.DMA
    shapes = (
        jax.ShapeDtypeStruct((rows, local), f32),
        jax.ShapeDtypeStruct((width, local), bf16),
        jax.ShapeDtypeStruct((rows, local), f32),
        jax.ShapeDtypeStruct((rank, local), f32),
        jax.ShapeDtypeStruct((rank, local), f32),
        jax.ShapeDtypeStruct((rows, local), f32),
        jax.ShapeDtypeStruct((local, width), bf16),
        jax.ShapeDtypeStruct((rows, local), f32),
        jax.ShapeDtypeStruct((local, rank), f32),
        jax.ShapeDtypeStruct((local, rank), f32),
    )
    out = pl.pallas_call(
        functools.partial(kernel, scaling, entries),
        out_shape=shapes,
        in_specs=[hbm] * 12,
        out_specs=(vmem,) * len(shapes),
        scratch_shapes=[
            pltpu.VMEM((tokens, width), bf16),
            pltpu.VMEM((tokens, width), bf16),
            pltpu.VMEM((tokens, local), bf16),
            pltpu.VMEM((tokens, local), bf16),
            pltpu.VMEM((2, devices, rows, rank), bf16),
            pltpu.VMEM((2, rows, local), f32),
            pltpu.VMEM((devices, 2, rows, local), bf16),
            pltpu.VMEM((2, local, width), f32),
            pltpu.VMEM((2, NY, quarter, rank), f32),
            pltpu.VMEM((2, NY - 1, quarter, rank), f32),
            pltpu.VMEM((NZ, piece, rank), f32),
            pltpu.VMEM((NZ - 1, piece, rank), f32),
            pltpu.VMEM((NY, NZ, piece, rank), bf16),
            pltpu.VMEM((NX * NC, 1, 128), f32),
            pltpu.VMEM((NY, 1, 128), f32),
            pltpu.VMEM((2, local, rank), f32),
            pltpu.VMEM((2, rank, local), f32),
            pltpu.VMEM((2, local, rank), f32),
            dma((9,)),
            dma((2, CHUNKS)),
            *[dma((NZ - 1,))] * 2,
            *[dma((NZ, NY - 1))] * 2,
            *[dma((NZ, 2))] * 2,
            *[dma((NZ,))] * 2,
            *[dma((2, NY - 1))] * 2,
            *[dma((NZ - 1,))] * 4,
            *[dma((NY - 1,))] * 2,
            *[dma((NX * NC - 1,))] * 2,
            *[dma((NY - 1,))] * 2,
            *[dma((NZ - 1,))] * 2,
            *[dma((NZ, NY - 1))] * 2,
        ],
        compiler_params=pltpu.CompilerParams(
            collective_id=0, has_side_effects=True, vmem_limit_bytes=32 * 1024 * 1024
        ),
    )(
        *(
            pltpu.with_memory_space_constraint(a, pltpu.HBM)
            for a in (
                block_input,
                value_cotangent,
                mixed_output,
                output_cotangent,
                value_basis,
                output_basis,
                value_weight,
                output_weight.T,
                value_mean,
                value_square,
                output_mean,
                output_square,
            )
        )
    )
    out = pl.pallas_call(
        store,
        out_shape=shapes,
        in_specs=[vmem] * len(shapes),
        out_specs=(vmem,) * len(shapes),
        compiler_params=pltpu.CompilerParams(vmem_limit_bytes=16 * 1024 * 1024),
    )(*out)
    out = list(out)
    out[5], out[7] = out[5].T, out[7].T
    return tuple(out)


def solution(mesh):
    return jax.shard_map(
        on_device,
        mesh=mesh,
        in_specs=(
            P("fs", None),
            P("fs", "tp"),
            P("fs", "tp"),
            P("fs", None),
            P("fs", "tp"),
            P("tp", "fs"),
            P("fs", None),
            P("fs", None),
            P(None, "tp"),
            P(None, "tp"),
            P("tp", None),
            P("tp", None),
        ),
        out_specs=(
            P("fs", "tp"),
            P(None, "tp"),
            P("fs", "tp"),
            P(None, "tp"),
            P(None, "tp"),
            P("tp", "fs"),
            P("tp", None),
            P("tp", "fs"),
            P("tp", None),
            P("tp", None),
        ),
        check_vma=False,
    )
```
